32 devices in a mesh: rep: 4 (over z), fs: 4 (over y, x), tp: 2 (over core).
Axes of the slice: x: 2, y: 2, z: 4, core: 2. Of those that a mesh axis runs over, the one named last changes fastest.
Arguments:
- hidden_pre: bfloat16 [8192, 4096], P(('rep', 'fs'), 'tp'), may hold values from -6 to 6
- out_grad: bfloat16 [8192, 2048], P(('rep', 'fs')), may hold values from -8 to 8
- down_weight: bfloat16 [2048, 4096], P('fs', 'tp'), may hold values from -0.09375 to 0.09375
Outputs:
- hidden_grad: bfloat16 [8192, 4096], P(('rep', 'fs'), 'tp')
- weight_grad: float32 [2048, 4096], P('fs', 'tp')
The draws below stay inside these ranges and needn't reach their ends.
All inputs are finite; a program needn't handle non-finite values.
Results may differ from the reference program's by a relative error of at most 0.0049.
Values may be sent and summed in bfloat16 or wider, within the bound.
A program may use at most 64 MiB of HBM per device.

```python
import jax
import jax.numpy as jnp
from jax import lax

D = 2048
FF = 4096
TOK_DEV = 512
TOKENS = 8192


def strengthened(array, key, source, target, shards_of, factor):
    def block_of(axis_at):
        return (jnp.arange(array.shape[axis_at]) // (array.shape[axis_at] // shards_of)).reshape((-1,) + (1,) * (array.ndim - 1 - axis_at))

    one_side = jax.random.permutation(key, shards_of)[block_of(target)]
    far = (block_of(target) + shards_of // 2) % shards_of
    return jnp.where((block_of(source) == one_side) | (block_of(source) == far), factor * array, array)


def level_of(key, dims, split, low, largest):
    def one(axis_at, parts):
        draws = jax.random.uniform(jax.random.fold_in(jax.random.fold_in(key, 6), axis_at), (parts,), jnp.float32, low / len(split), largest / len(split))
        return jnp.repeat(jnp.exp(draws), dims[axis_at] // parts).reshape((-1,) + (1,) * (len(dims) - axis_at - 1))

    level = one(*split[0])
    for cut in split[1:]:
        level = level * one(*cut)
    return level


def bell_draw(stream_key, shape, deviation, most, split=(), held_as=jnp.bfloat16):
    entries = deviation * jax.random.normal(stream_key, shape, jnp.float32)
    if split:
        entries = entries * level_of(stream_key, shape, split, -0.22, 0.18)
    return jnp.clip(entries, -most, most).astype(held_as)


def gaussian_with(key, dims, scale, limit, shards, heavy, held_as=jnp.bfloat16):
    result = scale * jax.random.normal(key, dims, jnp.float32)
    if shards:
        result = result * level_of(key, dims, shards, -0.22, 0.18)
    return jnp.clip(strengthened(result, jax.random.fold_in(key, 3), *heavy), -limit, limit).astype(held_as)


def setup_inputs(seed: int = 0) -> dict:
    key_list = jax.random.split(jax.random.key(seed), 4)
    hidden_pre = bell_draw(key_list[0], (TOKENS, FF), 1.0, 6.0, ((0, 16), (1, 2)))
    out_grad = gaussian_with(key_list[1], (TOKENS, D), 1.0, 8.0, ((0, 16),), (0, 1, 16, 2.0))
    down_weight = bell_draw(key_list[2], (D, FF), FF ** -0.5, 0.09375, ((0, 4), (1, 2)))
    return dict(hidden_pre=hidden_pre, out_grad=out_grad, down_weight=down_weight)


def reference(hidden_pre, out_grad, down_weight):
    count = TOKENS // TOK_DEV
    pre_blocks = hidden_pre.reshape(count, TOK_DEV, FF)
    grad_blocks = out_grad.reshape(count, TOK_DEV, D)

    def one_block(total, inputs):
        pre_rows, grad_rows = inputs
        positive = jnp.maximum(pre_rows.astype(jnp.float32), jnp.float32(0.0))
        back = jnp.dot(grad_rows, down_weight, preferred_element_type=jnp.float32)
        hidden_rows = (2.0 * positive * back).astype(jnp.bfloat16)
        act = (positive * positive).astype(jnp.bfloat16)
        part = lax.dot_general(grad_rows, act, (((0,), (0,)), ((), ())), preferred_element_type=jnp.float32)
        part = part.astype(jnp.bfloat16)
        return total + part.astype(jnp.float32), hidden_rows

    start = jnp.zeros((D, FF), jnp.float32)
    total, hidden_rows = lax.scan(one_block, start, (pre_blocks, grad_blocks))
    hidden_grad = hidden_rows.reshape(TOKENS, FF)
    weight_grad = total * jnp.float32(TOKENS ** -0.5)
    return hidden_grad, weight_grad
```

```python
import math

import jax
import jax.numpy as jnp
from jax import lax
from jax.experimental import pallas as pl
from jax.experimental.pallas import tpu as pltpu
from jax.sharding import PartitionSpec as P

MESH = pl.DeviceIdType.MESH
BF = jnp.bfloat16
F32 = jnp.float32


def plain_body(hidden_pre, out_grad, down_weight):
    rows = hidden_pre.shape[0]
    ff_local = hidden_pre.shape[1]
    back = jnp.dot(
        out_grad,
        lax.all_gather(down_weight, "fs", axis=0, tiled=True),
        preferred_element_type=F32,
    )
    positive = jnp.maximum(hidden_pre.astype(F32), 0.0)
    hidden_grad = (2.0 * positive * back).astype(BF)
    act = (positive * positive).astype(BF)
    partial_value = lax.dot_general(
        out_grad, act, (((0,), (0,)), ((), ())), preferred_element_type=F32
    )
    partial_value = partial_value.astype(BF)
    received = lax.all_to_all(partial_value, "fs", split_axis=0, concat_axis=0, tiled=True)
    groups = lax.axis_size("fs")
    local_sum = jnp.sum(
        received.reshape(groups, received.shape[0] // groups, ff_local), axis=0, dtype=F32
    )
    total = lax.psum(local_sum, "rep")
    tokens_all = rows * lax.axis_size("rep") * groups
    return (hidden_grad, total * (1.0 / math.sqrt(tokens_all)))


STEPS = 4
PIECES = ((0, 0, 1), (0, 1, 1), (1, 0, 2), (2, 0, 2), (3, 0, 2))


def kernel(hp, og, w, hg_out, tot_out,
           ogcat, ogt, whalf, hpc, pbs, pbr, pbo, gs, gr, gown, zs, z1r, z2r, zt,
           l_og, l_w, l_hp,
           og_s, og_r, od_s, od_r, w_s, w_r, fn_s, fm_s, f_r, pb_s, pb_r,
           hp_s, hp_r, g_s, g_r, z1_s, z1_rs, z2_s, z2_rs, z3_s, z3_rs):
    rows, ff = hp.shape
    depth = w.shape[0]
    half = ff // 2
    fc = half // STEPS
    unit = fc // 2
    part = rows // 2
    piece_rows = depth // 2
    fs = lax.axis_index("fs")
    core = lax.axis_index("tp")
    z = lax.axis_index("rep")
    last = lax.axis_size("rep") - 1
    a, b = fs // 2, fs % 2
    znear = z + 1 - 2 * (z % 2)
    apeer = {"fs": (1 - a) * 2 + b}
    bpeer = {"fs": a * 2 + (1 - b)}
    cpeer = {"tp": 1 - core}
    znext = {"rep": znear}
    zmid = {"rep": last - z}
    outer = jnp.logical_or(z == 0, z == last)
    inner = jnp.logical_not(outer)
    token_peer = (apeer, bpeer)
    weight_peer = (bpeer, apeer)
    scale = 1.0 / math.sqrt(rows * lax.axis_size("rep") * lax.axis_size("fs"))
    count = len(PIECES)

    def remote(src, dst, ssem, rsem, peer):
        return pltpu.make_async_remote_copy(
            src_ref=src, dst_ref=dst, send_sem=ssem, recv_sem=rsem,
            device_id=peer, device_id_type=MESH)

    def cut(i, size):
        return pl.ds(pl.multiple_of(i * size, size), size)

    place = (b, a)
    mine = [cut(place[q], depth) for q in range(2)]
    theirs = [cut(1 - place[q], depth) for q in range(2)]
    far_block = lambda q, p: 2 * (1 - a) + p if q == 0 else 2 * p + 1 - b
    own_block = lambda q, p: 2 * a + p if q == 0 else 2 * p + b
    low = cut(core, part)
    mid = pl.ds(pl.multiple_of(rows + core * part, part), part)
    mid_other = pl.ds(pl.multiple_of(rows + (1 - core) * part, part), part)
    both = [(q, p) for q in range(2) for p in range(2)]
    halves = range(2)

    def their_rows(q, h):
        return cut(2 * (1 - place[q]) + h, piece_rows)

    def piece_cols(k):
        j, first, units = PIECES[k]
        return j, pl.ds(first * unit, units * unit)

    def hp_cols(q, k):
        j, first, units = PIECES[k]
        return pl.ds(q * half + j * fc + first * unit, units * unit)

    def chunk(q, j):
        return q * STEPS + j

    def load_og(q, p):
        return pltpu.make_async_copy(
            og.at[:, cut(own_block(q, p), depth)],
            ogcat.at[q, pl.ds(0, rows), pl.ds(p * depth, depth)], l_og.at[q, p])

    def load_w(c):
        return pltpu.make_async_copy(
            w.at[:, pl.ds(c * fc, fc)], whalf.at[c, mine[c // STEPS]], l_w.at[c])

    def load_hp(c):
        return pltpu.make_async_copy(hp.at[:, pl.ds(c * fc, fc)], hpc.at[0, c], l_hp.at[c])

    def send_og(q, p):
        return remote(og.at[low, cut(far_block(q, p), depth)],
                      ogcat.at[q, mid, cut(p, depth)],
                      og_s.at[q, p], og_r.at[q, p], token_peer[q])

    def pass_og(q, p, span):
        spot = ogcat.at[q, span, cut(p, depth)]
        return remote(spot, spot, od_s.at[q, p], od_r.at[q, p], cpeer)

    def send_w(q):
        return remote(w.at[:, cut(chunk(q, z), fc)], whalf.at[chunk(q, z), mine[q]],
                      w_s.at[q], w_r.at[q], weight_peer[q])

    def pass_w(q, j, peer, ssem):
        spot = whalf.at[chunk(q, j), theirs[q]]
        return remote(spot, spot, ssem.at[chunk(q, j)], f_r.at[chunk(q, j)], peer)

    def near_w(q, j):
        return pass_w(q, j, znext, fn_s)

    def mid_w(q, j):
        return pass_w(q, j, zmid, fm_s)

    def send_hp(q, k):
        j, cols = piece_cols(k)
        return remote(hp.at[:, hp_cols(q, k)], hpc.at[1, chunk(q, j), :, cols],
                      hp_s.at[q, k], hp_r.at[q, k], token_peer[q])

    def send_pb(q, j):
        c = chunk(q, j)
        return remote(pbs.at[c], pbr.at[c], pb_s.at[c], pb_r.at[c], token_peer[q])

    def strip(ref, q, k, h):
        j, cols = piece_cols(k)
        return ref.at[chunk(q, j), pl.ds(h * piece_rows, piece_rows), cols]

    def send_g(q, k, h):
        return remote(strip(gs, q, k, h), strip(gr, q, k, h),
                      g_s.at[q, k, h], g_r.at[q, k, h], weight_peer[q])

    def send_z1(q, k, h):
        return remote(strip(zs, q, k, h), strip(z1r, q, k, h),
                      z1_s.at[q, k, h], z1_rs.at[q, k, h], znext)

    def send_z2(q, k, h):
        return remote(strip(zs, q, k, h), strip(z2r, q, k, h),
                      z2_s.at[q, k, h], z2_rs.at[q, k, h], zmid)

    def send_z3(q, k, h):
        return remote(strip(zt, q, k, h), strip(zt, q, k, h),
                      z3_s.at[q, k, h], z3_rs.at[q, k, h], znext)

    def act_of(q, k):
        j, cols = piece_cols(k)
        held = hpc[:, chunk(q, j), :, cols]
        positive = jnp.maximum(held.reshape(2 * rows, held.shape[-1]).astype(F32), 0.0)
        return (positive * positive).astype(BF)

    def g_out(q, k, act):
        for h in halves:
            strip(gs, q, k, h)[...] = jnp.dot(
                ogt[q, their_rows(q, h), :], act, preferred_element_type=F32).astype(BF)
            send_g(q, k, h).start()

    def g_own(q, k, act):
        j, cols = piece_cols(k)
        gown[chunk(q, j), :, cols] = jnp.dot(
            ogt[q, mine[q], :], act, preferred_element_type=F32)

    def got_hp(q, k):
        if PIECES[k][1] == 0:
            load_hp(chunk(q, PIECES[k][0])).wait()
        send_hp(q, k).wait_recv()

    def g_step(k, then):
        for q in range(2):
            got_hp(q, k)
            act = act_of(q, k)
            g_out(q, k, act)
            for n in then:
                send_hp(q, n).start()
            g_own(q, k, act)

    def each(k):
        return [(q, h) for q in range(2) for h in halves]

    def z_a(k):
        for q, h in each(k):
            send_g(q, k, h).wait_recv()

            @pl.when(outer)
            def _():
                strip(zs, q, k, h)[...] = (
                    strip(gown, q, k, h)[...] + strip(gr, q, k, h)[...].astype(F32)).astype(BF)
                send_z1(q, k, h).start()

    def z_b(k):
        @pl.when(inner)
        def _():
            for q, h in each(k):
                send_z1(q, k, h).wait_recv()
                strip(zs, q, k, h)[...] = (
                    strip(gown, q, k, h)[...] + strip(gr, q, k, h)[...].astype(F32)
                    + strip(z1r, q, k, h)[...].astype(F32)).astype(BF)
                send_z2(q, k, h).start()

    def put_total(q, k, h, value):
        j, first, units = PIECES[k]
        tot_out[h * piece_rows:(h + 1) * piece_rows,
                q * half + j * fc + first * unit:q * half + j * fc + (first + units) * unit
                ] = value

    def z_c(k):
        @pl.when(inner)
        def _():
            for q, h in each(k):
                send_z2(q, k, h).wait_recv()
                value = (strip(zs, q, k, h)[...].astype(F32)
                         + strip(z2r, q, k, h)[...].astype(F32)).astype(BF)
                strip(zt, q, k, h)[...] = value
                send_z3(q, k, h).start()
                put_total(q, k, h, value)

    def z_d(k):
        @pl.when(outer)
        def _():
            for q, h in each(k):
                send_z3(q, k, h).wait_recv()
                put_total(q, k, h, strip(zt, q, k, h)[...])

    order = (z, znear, jnp.where(outer, last - znear, last - z), jnp.where(outer, last - z, last - znear))

    def w_first():
        for q in range(2):
            send_w(q).wait_recv()
            near_w(q, z).start()

            @pl.when(inner)
            def _():
                mid_w(q, z).start()

    def w_second():
        for q in range(2):
            @pl.when(inner)
            def _():
                mid_w(q, last - z).wait_recv()
                near_w(q, last - z).start()
                near_w(q, znear).wait_recv()
                mid_w(q, znear).start()

    def w_third():
        for q in range(2):
            @pl.when(inner)
            def _():
                mid_w(q, last - znear).wait_recv()
                near_w(q, last - znear).start()

    def got_w(q, i):
        if i == 1:
            @pl.when(outer)
            def _():
                near_w(q, order[1]).wait_recv()
        elif i > 1:
            @pl.when(outer)
            def _():
                near_w(q, order[i]).wait_recv()

    def back_one(q, i):
        c = chunk(q, order[i])
        got_w(q, i)
        pbs[c] = jnp.dot(ogcat[q, rows:2 * rows, :], whalf[c], preferred_element_type=F32).astype(BF)
        send_pb(q, order[i]).start()
        pbo[c] = jnp.dot(ogcat[q, 0:rows, :], whalf[c], preferred_element_type=F32)

    def back(i):
        for q in range(2):
            back_one(q, i)

    def finish(i):
        for q in range(2):
            c = chunk(q, order[i])
            send_pb(q, order[i]).wait_recv()
            positive = jnp.maximum(hpc[0, c].astype(F32), 0.0)
            hg_out[:, cut(c, fc)] = (2.0 * positive * (pbo[c] + pbr[c].astype(F32))).astype(BF)

    def og_arrive(far):
        for q in range(2):
            p = 1 - place[q] if far else place[q]
            send_og(q, p).wait_recv()
            pass_og(q, p, mid).start()
        for q in range(2):
            p = 1 - place[q] if far else place[q]
            pass_og(q, p, mid_other).wait_recv()
            ogt[q, cut(p, depth), rows:2 * rows] = ogcat[q, rows:2 * rows, cut(p, depth)].T

    barrier = pltpu.get_barrier_semaphore()
    for peer in (apeer, bpeer, cpeer, znext, zmid):
        pl.semaphore_signal(barrier, inc=1, device_id=peer, device_id_type=MESH)
    for q, p in both:
        load_og(q, p).start()
    pl.semaphore_wait(barrier, 5)
    for q in range(2):
        send_w(q).start()
    for q in range(2):
        send_og(q, 1 - place[q]).start()
    for q in range(2):
        send_hp(q, 0).start()
    for q in range(2):
        send_og(q, place[q]).start()
    for k in (1, 2):
        for q in range(2):
            send_hp(q, k).start()
    for c in range(2 * STEPS):
        load_hp(c).start()
    for c in range(2 * STEPS):
        load_w(c).start()
    for q, p in both:
        load_og(q, p).wait()
    for q in range(2):
        ogt[q, :, 0:rows] = ogcat[q, 0:rows, :].T
    w_first()
    og_arrive(True)
    for q in range(2):
        got_hp(q, 0)
        g_out(q, 0, act_of(q, 0))
    w_second()
    og_arrive(False)
    for q in range(2):
        g_own(q, 0, act_of(q, 0))
    for c in range(2 * STEPS):
        load_w(c).wait()
    g_step(1, (3,))
    w_third()
    z_a(0)
    g_step(2, (4,))
    z_b(0)
    z_a(1)
    z_b(1)
    g_step(3, ())
    z_c(0)
    z_a(2)
    z_c(1)
    z_b(2)
    g_step(4, ())
    back(0)
    z_c(2)
    z_a(3)
    z_b(3)
    back(1)
    z_a(4)
    z_c(3)
    z_b(4)
    back(2)
    back(3)
    finish(0)
    z_c(4)
    for k in range(count - 1):
        z_d(k)
    finish(1)
    finish(2)
    z_d(count - 1)
    finish(3)

    for q, p in both:
        send_og(q, p).wait_send()
        pass_og(q, p, mid).wait_send()
    for q in range(2):
        send_w(q).wait_send()
        near_w(q, z).wait_send()
        for k in range(count):
            send_hp(q, k).wait_send()
        for j in range(STEPS):
            send_pb(q, j).wait_send()
    pieces = [(q, k, h) for k in range(count) for q in range(2) for h in halves]
    for q, k, h in pieces:
        send_g(q, k, h).wait_send()

    @pl.when(outer)
    def _():
        for q, k, h in pieces:
            send_z1(q, k, h).wait_send()

    @pl.when(inner)
    def _():
        for q in range(2):
            mid_w(q, z).wait_send()
            mid_w(q, znear).wait_send()
            near_w(q, last - z).wait_send()
            near_w(q, last - znear).wait_send()
        for q, k, h in pieces:
            send_z2(q, k, h).wait_send()
            send_z3(q, k, h).wait_send()


def paired_body(hidden_pre, out_grad, down_weight):
    rows, ff = hidden_pre.shape
    depth = down_weight.shape[0]
    chunks = 2 * STEPS
    fc = ff // chunks
    count = len(PIECES)
    any_spec = pl.BlockSpec(memory_space=pl.ANY)
    vmem_spec = pl.BlockSpec(memory_space=pltpu.VMEM)

    def block(r, dtype):
        return pltpu.VMEM((chunks, r, fc), dtype)

    sem = pltpu.SemaphoreType.DMA
    hidden_grad, total = pl.pallas_call(
        kernel,
        out_shape=(jax.ShapeDtypeStruct((rows, ff), BF), jax.ShapeDtypeStruct((depth, ff), BF)),
        in_specs=[any_spec] * 3,
        out_specs=(vmem_spec, vmem_spec),
        scratch_shapes=[
            pltpu.VMEM((2, 2 * rows, 2 * depth), BF),
            pltpu.VMEM((2, 2 * depth, 2 * rows), BF),
            block(2 * depth, BF),
            pltpu.VMEM((2, chunks, rows, fc), BF),
            block(rows, BF), block(rows, BF), block(rows, F32),
            block(depth, BF), block(depth, BF), block(depth, F32),
            block(depth, BF), block(depth, BF), block(depth, BF), block(depth, BF),
            sem((2, 2)), sem((chunks,)), sem((chunks,)),
        ] + [sem((2, 2))] * 4 + [sem((2,))] * 2 + [sem((chunks,))] * 5
        + [sem((2, count))] * 2 + [sem((2, count, 2))] * 8,
        compiler_params=pltpu.CompilerParams(
            collective_id=0, has_side_effects=True, vmem_limit_bytes=48 * 1024 * 1024
        ),
    )(hidden_pre, out_grad, down_weight)
    tokens_all = rows * lax.axis_size("rep") * lax.axis_size("fs")
    return hidden_grad, total.astype(F32) * (1.0 / math.sqrt(tokens_all))


def solution(mesh):
    placed = (P(("rep", "fs"), "tp"), P(("rep", "fs"), None), P("fs", "tp"))
    two_by_two = mesh.shape["fs"] == 4 and mesh.shape["tp"] == 2 and mesh.shape["rep"] == 4
    return jax.shard_map(
        paired_body if two_by_two else plain_body,
        mesh=mesh,
        in_specs=placed,
        out_specs=(P(("rep", "fs"), "tp"), P("fs", "tp")),
        check_vma=False,
    )
```

```python
import math

import jax
import jax.numpy as jnp
from jax import lax
from jax.experimental import pallas as pl
from jax.experimental.pallas import tpu as pltpu
from jax.sharding import PartitionSpec as P

MESH = pl.DeviceIdType.MESH
BF = jnp.bfloat16
F32 = jnp.float32


def plain_body(hidden_pre, out_grad, down_weight):
    rows = hidden_pre.shape[0]
    ff_local = hidden_pre.shape[1]
    back = jnp.dot(
        out_grad,
        lax.all_gather(down_weight, "fs", axis=0, tiled=True),
        preferred_element_type=F32,
    )
    positive = jnp.maximum(hidden_pre.astype(F32), 0.0)
    hidden_grad = (2.0 * positive * back).astype(BF)
    act = (positive * positive).astype(BF)
    partial_value = lax.dot_general(
        out_grad, act, (((0,), (0,)), ((), ())), preferred_element_type=F32
    )
    partial_value = partial_value.astype(BF)
    received = lax.all_to_all(partial_value, "fs", split_axis=0, concat_axis=0, tiled=True)
    groups = lax.axis_size("fs")
    local_sum = jnp.sum(
        received.reshape(groups, received.shape[0] // groups, ff_local), axis=0, dtype=F32
    )
    total = lax.psum(local_sum, "rep")
    tokens_all = rows * lax.axis_size("rep") * groups
    return (hidden_grad, total * (1.0 / math.sqrt(tokens_all)))


STEPS = 4
PIECES = ((0, 0, 1), (0, 1, 1), (1, 0, 2), (2, 0, 2), (3, 0, 2))
PUTS = 4
PARTS = 2
WPARTS = 2
PLAN = (
    ("sw", 1, 0), ("sw", 0, 1), ("sw", 0, 0), ("sw", 1, 1), ("sog", 0, 1), ("sog", 0, 0), ("sog", 1, 1),
    ("w1", 1, 0), ("tr0", 1), ("w1", 0, 0), ("shp", 0, 3), ("sog", 1, 0), ("w2b", 1, 0), ("w1", 1, 1),
    ("shp", 0, 1), ("shp", 1, 1), ("w2a", 1, 0), ("w2b", 1, 1), ("w3", 1, 0), ("w1", 0, 1), ("w2a", 0, 0),
    ("shp", 1, 2), ("ogr", 1, 1), ("ogr", 0, 1), ("tr0", 0), ("w2b", 0, 1), ("ogr", 1, 0), ("ogr", 0, 0),
    ("w2a", 1, 1), ("ogt", 0, 1), ("ogt", 1, 1), ("shp", 0, 0), ("gout", 1, 1), ("ogt", 0, 0),
    ("gout", 0, 3), ("shp", 0, 2), ("w3", 1, 1), ("w2a", 0, 1), ("w2b", 0, 0), ("gown", 0, 3),
    ("gout", 1, 2), ("gout", 0, 1), ("shp", 0, 4), ("ogt", 1, 0), ("w3", 0, 0), ("za", 0, 3, 0),
    ("gout", 0, 0), ("za", 0, 3, 1), ("w3", 0, 1), ("shp", 1, 0), ("shp", 1, 3), ("zb", 0, 3, 0),
    ("zb", 0, 3, 1), ("gown", 0, 1), ("zc", 0, 3, 0), ("gown", 1, 1), ("za", 0, 1, 0), ("za", 0, 1, 1),
    ("za", 1, 1, 0), ("za", 1, 1, 1), ("zb", 0, 1, 0), ("zb", 0, 1, 1), ("gown", 1, 2), ("gout", 0, 2),
    ("zb", 1, 1, 1), ("shp", 1, 4), ("za", 1, 2, 0), ("za", 1, 2, 1), ("zb", 1, 1, 0), ("zc", 0, 3, 1),
    ("gown", 0, 0), ("zb", 1, 2, 0), ("zc", 0, 1, 1), ("gown", 0, 2), ("gout", 1, 0), ("za", 0, 0, 0),
    ("gout", 1, 3), ("za", 0, 0, 1), ("za", 0, 2, 0), ("zc", 1, 1, 1), ("bk", 0, 2), ("gown", 1, 0),
    ("zc", 1, 1, 0), ("zd", 0, 1, 1), ("za", 1, 0, 1), ("zd", 1, 1, 0), ("zb", 1, 2, 1), ("zc", 0, 1, 0),
    ("gown", 1, 3), ("za", 0, 2, 1), ("zc", 1, 2, 0), ("zb", 0, 0, 0), ("gout", 0, 4), ("zd", 0, 3, 1),
    ("zb", 0, 0, 1), ("zc", 1, 2, 1), ("bk", 1, 0), ("zb", 0, 2, 0), ("zb", 1, 0, 1), ("za", 1, 3, 0),
    ("zc", 0, 0, 1), ("bko", 0, 2), ("zc", 0, 0, 0), ("zb", 0, 2, 1), ("gout", 1, 4), ("za", 1, 3, 1),
    ("za", 1, 0, 0), ("zc", 0, 2, 0), ("zb", 1, 3, 0), ("zc", 0, 2, 1), ("bko", 1, 0), ("gown", 0, 4),
    ("gown", 1, 4), ("za", 0, 4, 1), ("za", 0, 4, 0), ("zd", 0, 2, 0), ("zb", 1, 3, 1), ("bk", 0, 1),
    ("bk", 1, 1), ("zc", 1, 0, 1), ("bk", 1, 3), ("bk", 0, 0), ("zc", 1, 3, 0), ("bko", 0, 1),
    ("zb", 0, 4, 1), ("za", 1, 4, 0), ("bko", 1, 1), ("zd", 0, 0, 1), ("za", 1, 4, 1), ("zc", 1, 3, 1),
    ("zd", 1, 0, 1), ("zb", 0, 4, 0), ("zd", 1, 3, 1), ("bk", 1, 2), ("zc", 0, 4, 1), ("zb", 1, 4, 0),
    ("zd", 0, 1, 0), ("bko", 1, 3), ("bk", 0, 3), ("fin", 1, 0), ("bko", 0, 3), ("zc", 0, 4, 0),
    ("zd", 0, 3, 0), ("bko", 0, 0), ("zb", 1, 4, 1), ("fin", 1, 1), ("bko", 1, 2), ("zb", 1, 0, 0),
    ("zc", 1, 4, 0), ("zd", 0, 0, 0), ("fin", 1, 3), ("zc", 1, 4, 1), ("zd", 0, 2, 1), ("fin", 0, 2),
    ("fin", 0, 1), ("fin", 0, 0), ("zd", 1, 4, 1), ("zd", 1, 2, 1), ("zc", 1, 0, 0), ("zd", 1, 1, 1),
    ("zd", 1, 3, 0), ("zd", 0, 4, 0), ("zd", 1, 4, 0), ("fin", 0, 3), ("zd", 1, 2, 0), ("fin", 1, 2),
    ("zd", 0, 4, 1), ("zd", 1, 0, 0),
)


def kernel(hp, og, w, hg_out, tot_out,
           ogcat, ogt, whalf, hpc, pbs, pbr, pbo, gs, gr, gown, zs, z1r, z2r, zt,
           l_og, l_w, l_hp,
           og_s, og_r, od_s, od_r, w_s, w_r, fn_s, fm_s, f_r, pb_s, pb_r,
           hp_s, hp_r, g_s, g_r, z1_s, z1_rs, z2_s, z2_rs, z3_s, z3_rs):
    rows, ff = hp.shape
    depth = w.shape[0]
    half = ff // 2
    fc = half // STEPS
    unit = fc // 2
    part = rows // 2
    w_rows = depth // WPARTS
    piece_rows = depth // PARTS
    fs = lax.axis_index("fs")
    core = lax.axis_index("tp")
    z = lax.axis_index("rep")
    last = lax.axis_size("rep") - 1
    a, b = fs // 2, fs % 2
    znear = z + 1 - 2 * (z % 2)
    apeer = {"fs": (1 - a) * 2 + b}
    bpeer = {"fs": a * 2 + (1 - b)}
    cpeer = {"tp": 1 - core}
    znext = {"rep": znear}
    zmid = {"rep": last - z}
    outer = jnp.logical_or(z == 0, z == last)
    inner = jnp.logical_not(outer)
    token_peer = (apeer, bpeer)
    weight_peer = (bpeer, apeer)
    scale = 1.0 / math.sqrt(rows * lax.axis_size("rep") * lax.axis_size("fs"))
    count = len(PIECES)

    def remote(src, dst, ssem, rsem, peer):
        return pltpu.make_async_remote_copy(
            src_ref=src, dst_ref=dst, send_sem=ssem, recv_sem=rsem,
            device_id=peer, device_id_type=MESH)

    def cut(i, size):
        return pl.ds(pl.multiple_of(i * size, size), size)

    place = (b, a)
    mine = [cut(place[q], depth) for q in range(2)]
    theirs = [cut(1 - place[q], depth) for q in range(2)]
    far_block = lambda q, p: 2 * (1 - a) + p if q == 0 else 2 * p + 1 - b
    own_block = lambda q, p: 2 * a + p if q == 0 else 2 * p + b
    low = cut(core, part)
    mid = pl.ds(pl.multiple_of(rows + core * part, part), part)
    mid_other = pl.ds(pl.multiple_of(rows + (1 - core) * part, part), part)
    both = [(q, p) for q in range(2) for p in range(2)]
    halves = range(PARTS)

    def their_rows(q, h):
        return cut(PARTS * (1 - place[q]) + h, piece_rows)

    def piece_cols(k):
        j, first, units = PIECES[k]
        return j, pl.ds(first * unit, units * unit)

    def hp_cols(q, k):
        j, first, units = PIECES[k]
        return pl.ds(q * half + j * fc + first * unit, units * unit)

    def chunk(q, j):
        return q * STEPS + j

    def load_og(q, p):
        return pltpu.make_async_copy(
            og.at[:, cut(own_block(q, p), depth)],
            ogcat.at[q, pl.ds(0, rows), pl.ds(p * depth, depth)], l_og.at[q, p])

    def load_w(c):
        return pltpu.make_async_copy(
            w.at[:, pl.ds(c * fc, fc)], whalf.at[c, mine[c // STEPS]], l_w.at[c])

    def load_hp(c):
        return pltpu.make_async_copy(hp.at[:, pl.ds(c * fc, fc)], hpc.at[0, c], l_hp.at[c])

    def send_og(q, p):
        return remote(og.at[low, cut(far_block(q, p), depth)],
                      ogcat.at[q, mid, cut(p, depth)],
                      og_s.at[q, p], og_r.at[q, p], token_peer[q])

    def pass_og(q, p, span):
        spot = ogcat.at[q, span, cut(p, depth)]
        return remote(spot, spot, od_s.at[q, p], od_r.at[q, p], cpeer)

    def send_w(q, h):
        c = chunk(q, z)
        return remote(w.at[h * w_rows:(h + 1) * w_rows, cut(c, fc)],
                      whalf.at[c, cut(WPARTS * place[q] + h, w_rows)],
                      w_s.at[q, h], w_r.at[q, h], weight_peer[q])

    def pass_w(q, j, h, peer, ssem):
        c = chunk(q, j)
        spot = whalf.at[c, cut(WPARTS * (1 - place[q]) + h, w_rows)]
        return remote(spot, spot, ssem.at[c, h], f_r.at[c, h], peer)

    def near_w(q, j, h):
        return pass_w(q, j, h, znext, fn_s)

    def mid_w(q, j, h):
        return pass_w(q, j, h, zmid, fm_s)

    def send_hp(q, k):
        j, cols = piece_cols(k)
        return remote(hp.at[:, hp_cols(q, k)], hpc.at[1, chunk(q, j), :, cols],
                      hp_s.at[q, k], hp_r.at[q, k], token_peer[q])

    def send_pb(q, j):
        c = chunk(q, j)
        return remote(pbs.at[c], pbr.at[c], pb_s.at[c], pb_r.at[c], token_peer[q])

    def strip(ref, q, k, h):
        j, cols = piece_cols(k)
        return ref.at[chunk(q, j), pl.ds(h * piece_rows, piece_rows), cols]

    def send_g(q, k, h):
        return remote(strip(gs, q, k, h), strip(gr, q, k, h),
                      g_s.at[q, k, h], g_r.at[q, k, h], weight_peer[q])

    def send_z1(q, k, h):
        return remote(strip(zs, q, k, h), strip(z1r, q, k, h),
                      z1_s.at[q, k, h], z1_rs.at[q, k, h], znext)

    def send_z2(q, k, h):
        return remote(strip(zs, q, k, h), strip(z2r, q, k, h),
                      z2_s.at[q, k, h], z2_rs.at[q, k, h], zmid)

    def send_z3(q, k, h):
        return remote(strip(zt, q, k, h), strip(zt, q, k, h),
                      z3_s.at[q, k, h], z3_rs.at[q, k, h], znext)

    def act_of(q, k):
        j, cols = piece_cols(k)
        held = hpc[:, chunk(q, j), :, cols]
        positive = jnp.maximum(held.reshape(2 * rows, held.shape[-1]).astype(F32), 0.0)
        return (positive * positive).astype(BF)

    def g_out(q, k, act):
        for h in halves:
            strip(gs, q, k, h)[...] = jnp.dot(
                ogt[q, their_rows(q, h), :], act, preferred_element_type=F32).astype(BF)
            send_g(q, k, h).start()

    def g_own(q, k, act):
        j, cols = piece_cols(k)
        gown[chunk(q, j), :, cols] = jnp.dot(
            ogt[q, mine[q], :], act, preferred_element_type=F32)

    loaded = set()

    def once(name, copies):
        if name not in loaded:
            loaded.add(name)
            for copy in copies():
                copy.wait()

    def transpose_own(q):
        once("og", lambda: [load_og(*at) for at in both])
        ogt[q, :, 0:rows] = ogcat[q, 0:rows, :].T

    def og_part(q, far):
        return 1 - place[q] if far else place[q]

    def og_relay(q, far):
        p = og_part(q, far)
        send_og(q, p).wait_recv()
        pass_og(q, p, mid).start()

    def og_whole(q, far):
        p = og_part(q, far)
        pass_og(q, p, mid_other).wait_recv()
        ogt[q, cut(p, depth), rows:2 * rows] = ogcat[q, rows:2 * rows, cut(p, depth)].T

    def grad_send(q, k):
        c = chunk(q, PIECES[k][0])
        once(c, lambda: [load_hp(c)])
        send_hp(q, k).wait_recv()
        g_out(q, k, act_of(q, k))

    def grad_keep(q, k):
        g_own(q, k, act_of(q, k))

    def z_outer_send(q, k, h):
        send_g(q, k, h).wait_recv()
        strip(zs, q, k, h)[...] = (
            strip(gown, q, k, h)[...] + strip(gr, q, k, h)[...].astype(F32)).astype(BF)
        send_z1(q, k, h).start()

    def z_inner_send(q, k, h):
        send_g(q, k, h).wait_recv()
        send_z1(q, k, h).wait_recv()
        strip(zs, q, k, h)[...] = (
            strip(gown, q, k, h)[...] + strip(gr, q, k, h)[...].astype(F32)
            + strip(z1r, q, k, h)[...].astype(F32)).astype(BF)
        send_z2(q, k, h).start()

    def put_total(q, k, h, value):
        j, first, units = PIECES[k]
        tot_out[h * piece_rows:(h + 1) * piece_rows,
                q * half + j * fc + first * unit:q * half + j * fc + (first + units) * unit
                ] = value

    def z_inner_last(q, k, h):
        send_z2(q, k, h).wait_recv()
        value = (strip(zs, q, k, h)[...].astype(F32)
                 + strip(z2r, q, k, h)[...].astype(F32)).astype(BF)
        strip(zt, q, k, h)[...] = value
        send_z3(q, k, h).start()
        put_total(q, k, h, value)

    def z_outer_last(q, k, h):
        send_z3(q, k, h).wait_recv()
        put_total(q, k, h, strip(zt, q, k, h)[...])

    order = (z, znear, jnp.where(outer, last - znear, last - z), jnp.where(outer, last - z, last - znear))

    def w_own(q, h):
        send_w(q, h).wait_recv()
        near_w(q, z, h).start()

        @pl.when(inner)
        def _():
            mid_w(q, z, h).start()

    def w_down(q, h):
        mid_w(q, last - z, h).wait_recv()
        near_w(q, last - z, h).start()

    def w_across(q, h):
        near_w(q, znear, h).wait_recv()
        mid_w(q, znear, h).start()

    def w_far(q, h):
        mid_w(q, last - znear, h).wait_recv()
        near_w(q, last - znear, h).start()

    def back_send(q, i):
        once("w", lambda: [load_w(c) for c in range(2 * STEPS)])
        c = chunk(q, order[i])
        if i > 0:
            @pl.when(outer)
            def _():
                for h in range(WPARTS):
                    near_w(q, order[i], h).wait_recv()
        pbs[c] = jnp.dot(ogcat[q, rows:2 * rows, :], whalf[c], preferred_element_type=F32).astype(BF)
        send_pb(q, order[i]).start()

    def back_keep(q, i):
        c = chunk(q, order[i])
        pbo[c] = jnp.dot(ogcat[q, 0:rows, :], whalf[c], preferred_element_type=F32)

    def finish(q, i):
        c = chunk(q, order[i])
        send_pb(q, order[i]).wait_recv()
        positive = jnp.maximum(hpc[0, c].astype(F32), 0.0)
        hg_out[:, cut(c, fc)] = (2.0 * positive * (pbo[c] + pbr[c].astype(F32))).astype(BF)

    shared = {
        "sw": lambda q, h: send_w(q, h).start(),
        "sog": lambda q, far: send_og(q, og_part(q, far)).start(),
        "shp": lambda q, k: send_hp(q, k).start(),
        "tr0": transpose_own, "ogr": og_relay, "ogt": og_whole,
        "gout": grad_send, "gown": grad_keep, "w1": w_own,
        "bk": back_send, "bko": back_keep, "fin": finish,
    }
    at_outer = {"za": z_outer_send, "zd": z_outer_last}
    at_inner = {"zb": z_inner_send, "zc": z_inner_last, "w2a": w_down, "w2b": w_across, "w3": w_far}

    def run_group(table, role, group):
        steps = [(table[name], args) for name, *args in group if name in table]
        if steps:
            @pl.when(role)
            def _():
                for act, args in steps:
                    act(*args)

    barrier = pltpu.get_barrier_semaphore()
    for peer in (apeer, bpeer, cpeer, znext, zmid):
        pl.semaphore_signal(barrier, inc=1, device_id=peer, device_id_type=MESH)
    for q, p in both:
        load_og(q, p).start()
    pl.semaphore_wait(barrier, 5)
    group = []
    started = False
    for step in PLAN:
        if step[0] in shared:
            run_group(at_outer, outer, group)
            run_group(at_inner, inner, group)
            group = []
            if not started and step[0] == "tr0":
                started = True
                for c in range(2 * STEPS):
                    load_hp(c).start()
                for c in range(2 * STEPS):
                    load_w(c).start()
            shared[step[0]](*step[1:])
        else:
            group.append(step)
    run_group(at_outer, outer, group)
    run_group(at_inner, inner, group)

    for q, p in both:
        send_og(q, p).wait_send()
        pass_og(q, p, mid).wait_send()
    for q in range(2):
        for h in range(WPARTS):
            send_w(q, h).wait_send()
            near_w(q, z, h).wait_send()
        for k in range(count):
            send_hp(q, k).wait_send()
        for j in range(STEPS):
            send_pb(q, j).wait_send()
    pieces = [(q, k, h) for k in range(count) for q in range(2) for h in halves]
    for q, k, h in pieces:
        send_g(q, k, h).wait_send()

    @pl.when(outer)
    def _():
        for q, k, h in pieces:
            send_z1(q, k, h).wait_send()

    @pl.when(inner)
    def _():
        for q in range(2):
            for h in range(WPARTS):
                mid_w(q, z, h).wait_send()
                mid_w(q, znear, h).wait_send()
                near_w(q, last - z, h).wait_send()
                near_w(q, last - znear, h).wait_send()
        for q, k, h in pieces:
            send_z2(q, k, h).wait_send()
            send_z3(q, k, h).wait_send()


def put_kernel(hg, total, hg_out, tot_out, wide, sems):
    size = hg.shape[0] // PUTS
    tokens_all = size * PUTS * lax.axis_size("rep") * lax.axis_size("fs")
    copies = []
    for i in range(PUTS):
        span = pl.ds(i * size, size)
        copies.append(pltpu.make_async_copy(hg.at[span], hg_out.at[span], sems.at[1, i]))
        copies[-1].start()
        wide[span] = total[span].astype(F32) * (1.0 / math.sqrt(tokens_all))
        copies.append(pltpu.make_async_copy(wide.at[span], tot_out.at[span], sems.at[0, i]))
        copies[-1].start()
    for copy in copies:
        copy.wait()


def paired_body(hidden_pre, out_grad, down_weight):
    rows, ff = hidden_pre.shape
    depth = down_weight.shape[0]
    chunks = 2 * STEPS
    fc = ff // chunks
    count = len(PIECES)
    any_spec = pl.BlockSpec(memory_space=pl.ANY)
    vmem_spec = pl.BlockSpec(memory_space=pltpu.VMEM)

    def block(r, dtype):
        return pltpu.VMEM((chunks, r, fc), dtype)

    sem = pltpu.SemaphoreType.DMA
    hidden_grad, total = pl.pallas_call(
        kernel,
        out_shape=(jax.ShapeDtypeStruct((rows, ff), BF), jax.ShapeDtypeStruct((depth, ff), BF)),
        in_specs=[any_spec] * 3,
        out_specs=(vmem_spec, vmem_spec),
        scratch_shapes=[
            pltpu.VMEM((2, 2 * rows, 2 * depth), BF),
            pltpu.VMEM((2, 2 * depth, 2 * rows), BF),
            block(2 * depth, BF),
            pltpu.VMEM((2, chunks, rows, fc), BF),
            block(rows, BF), block(rows, BF), block(rows, F32),
            block(depth, BF), block(depth, BF), block(depth, F32),
            block(depth, BF), block(depth, BF), block(depth, BF), block(depth, BF),
            sem((2, 2)), sem((chunks,)), sem((chunks,)),
        ] + [sem((2, 2))] * 4 + [sem((2, WPARTS))] * 2 + [sem((chunks, WPARTS))] * 3 + [sem((chunks,))] * 2
        + [sem((2, count))] * 2 + [sem((2, count, PARTS))] * 8,
        compiler_params=pltpu.CompilerParams(
            collective_id=0, has_side_effects=True, vmem_limit_bytes=48 * 1024 * 1024
        ),
    )(hidden_pre, out_grad, down_weight)
    return pl.pallas_call(
        put_kernel,
        out_shape=(jax.ShapeDtypeStruct((rows, ff), BF), jax.ShapeDtypeStruct((depth, ff), F32)),
        in_specs=[any_spec, vmem_spec],
        out_specs=(any_spec, any_spec),
        scratch_shapes=[pltpu.VMEM((depth, ff), F32), pltpu.SemaphoreType.DMA((2, PUTS))],
        compiler_params=pltpu.CompilerParams(vmem_limit_bytes=8 * 1024 * 1024),
    )(hidden_grad, total)


def solution(mesh):
    placed = (P(("rep", "fs"), "tp"), P(("rep", "fs"), None), P("fs", "tp"))
    two_by_two = mesh.shape["fs"] == 4 and mesh.shape["tp"] == 2 and mesh.shape["rep"] == 4
    return jax.shard_map(
        paired_body if two_by_two else plain_body,
        mesh=mesh,
        in_specs=placed,
        out_specs=(P(("rep", "fs"), "tp"), P("fs", "tp")),
        check_vma=False,
    )
```

```python
import math

import jax
import jax.numpy as jnp
from jax import lax
from jax.experimental import pallas as pl
from jax.experimental.pallas import tpu as pltpu
from jax.sharding import PartitionSpec as P

MESH = pl.DeviceIdType.MESH
BF = jnp.bfloat16
F32 = jnp.float32


def plain_body(hidden_pre, out_grad, down_weight):
    rows = hidden_pre.shape[0]
    ff_local = hidden_pre.shape[1]
    back = jnp.dot(
        out_grad,
        lax.all_gather(down_weight, "fs", axis=0, tiled=True),
        preferred_element_type=F32,
    )
    positive = jnp.maximum(hidden_pre.astype(F32), 0.0)
    hidden_grad = (2.0 * positive * back).astype(BF)
    act = (positive * positive).astype(BF)
    partial_value = lax.dot_general(
        out_grad, act, (((0,), (0,)), ((), ())), preferred_element_type=F32
    )
    partial_value = partial_value.astype(BF)
    received = lax.all_to_all(partial_value, "fs", split_axis=0, concat_axis=0, tiled=True)
    groups = lax.axis_size("fs")
    local_sum = jnp.sum(
        received.reshape(groups, received.shape[0] // groups, ff_local), axis=0, dtype=F32
    )
    total = lax.psum(local_sum, "rep")
    tokens_all = rows * lax.axis_size("rep") * groups
    return (hidden_grad, total * (1.0 / math.sqrt(tokens_all)))


STEPS = 4
PIECES = ((0, 0, 2), (1, 0, 2), (2, 0, 2), (3, 0, 2))
PUTS = 2
PARTS = 2
WPARTS = 2
PLAN = (
    ("sw", 0, 1), ("sw", 0, 0), ("sw", 1, 1), ("sog", 0, 1), ("sog", 1, 1), ("sw", 1, 0), ("sog", 1, 0),
    ("shp", 0, 3), ("w1", 1, 1), ("sog", 0, 0), ("w1", 0, 0), ("tr0", 0), ("ogr", 0, 1), ("w2b", 1, 1),
    ("shp", 0, 2), ("w1", 0, 1), ("shp", 1, 2), ("w1", 1, 0), ("w2b", 0, 0), ("w2a", 1, 1), ("ogr", 1, 1),
    ("w2b", 0, 1), ("ogt", 1, 1), ("w2a", 0, 0), ("w2b", 1, 0), ("ogt", 0, 1), ("ogr", 1, 0), ("w2a", 0, 1),
    ("gout", 0, 3), ("w2a", 1, 0), ("shp", 1, 0), ("ogr", 0, 0), ("tr0", 1), ("ogt", 1, 0), ("gout", 1, 2),
    ("w3", 0, 0), ("w3", 1, 1), ("w3", 1, 0), ("ogt", 0, 0), ("gown", 0, 3), ("shp", 0, 1), ("zb", 0, 3, 0),
    ("za", 0, 3, 0), ("za", 0, 3, 1), ("w3", 0, 1), ("gout", 0, 2), ("zb", 0, 3, 1), ("gown", 0, 2),
    ("shp", 1, 3), ("gown", 1, 2), ("za", 1, 2, 0), ("za", 1, 2, 1), ("gout", 1, 0), ("zc", 0, 3, 0),
    ("zb", 1, 2, 0), ("za", 0, 2, 0), ("za", 0, 2, 1), ("gown", 1, 0), ("zb", 1, 2, 1), ("zc", 0, 3, 1),
    ("zc", 1, 2, 0), ("zb", 0, 2, 0), ("shp", 0, 0), ("gout", 0, 1), ("gown", 0, 1), ("za", 1, 0, 0),
    ("zc", 1, 2, 1), ("zb", 0, 2, 1), ("shp", 1, 1), ("za", 1, 0, 1), ("gout", 1, 3), ("zc", 0, 2, 0),
    ("za", 0, 1, 0), ("zb", 1, 0, 0), ("bk", 0, 2), ("gown", 1, 3), ("zc", 0, 2, 1), ("zb", 1, 0, 1),
    ("za", 0, 1, 1), ("gout", 0, 0), ("bk", 1, 1), ("za", 1, 3, 0), ("bk", 1, 3), ("gown", 0, 0),
    ("zc", 1, 0, 0), ("za", 1, 3, 1), ("zb", 0, 1, 0), ("bko", 1, 1), ("zd", 0, 3, 1), ("bk", 1, 0),
    ("zb", 0, 1, 1), ("zc", 1, 0, 1), ("zd", 1, 2, 1), ("gout", 1, 1), ("gown", 1, 1), ("bk", 0, 1),
    ("za", 0, 0, 0), ("bko", 0, 2), ("zc", 0, 1, 0), ("zb", 1, 3, 0), ("bk", 0, 0), ("zb", 1, 3, 1),
    ("zc", 0, 1, 1), ("zc", 1, 3, 0), ("za", 0, 0, 1), ("zb", 0, 0, 0), ("za", 1, 1, 0), ("za", 1, 1, 1),
    ("zb", 0, 0, 1), ("zc", 1, 3, 1), ("zc", 0, 0, 0), ("zd", 1, 0, 0), ("fin", 0, 2), ("zb", 1, 1, 0),
    ("bk", 1, 2), ("bko", 0, 1), ("zc", 0, 0, 1), ("zb", 1, 1, 1), ("bk", 0, 3), ("zd", 0, 2, 1),
    ("zd", 1, 3, 1), ("bko", 1, 3), ("zd", 1, 0, 1), ("zc", 1, 1, 0), ("zd", 1, 3, 0), ("zd", 0, 1, 0),
    ("zd", 0, 3, 0), ("bko", 1, 0), ("zc", 1, 1, 1), ("zd", 1, 2, 0), ("bko", 0, 3), ("zd", 0, 0, 1),
    ("zd", 0, 0, 0), ("fin", 1, 0), ("zd", 0, 1, 1), ("bko", 0, 0), ("fin", 0, 1), ("fin", 1, 3),
    ("fin", 1, 1), ("bko", 1, 2), ("zd", 0, 2, 0), ("zd", 1, 1, 1), ("fin", 0, 0), ("zd", 1, 1, 0),
    ("fin", 1, 2), ("fin", 0, 3),
)


def kernel(hp, og, w, hg_out, tot_out,
           ogcat, ogt, whalf, hpc, pbs, pbr, pbo, gs, gr, gown, zs, z1r, z2r, zt,
           l_og, l_w, l_hp,
           og_s, og_r, od_s, od_r, w_s, w_r, fn_s, fm_s, f_r, pb_s, pb_r,
           hp_s, hp_r, g_s, g_r, z1_s, z1_rs, z2_s, z2_rs, z3_s, z3_rs):
    rows, ff = hp.shape
    depth = w.shape[0]
    half = ff // 2
    fc = half // STEPS
    unit = fc // 2
    part = rows // 2
    w_rows = depth // WPARTS
    piece_rows = depth // PARTS
    fs = lax.axis_index("fs")
    core = lax.axis_index("tp")
    z = lax.axis_index("rep")
    last = lax.axis_size("rep") - 1
    a, b = fs // 2, fs % 2
    znear = z + 1 - 2 * (z % 2)
    apeer = {"fs": (1 - a) * 2 + b}
    bpeer = {"fs": a * 2 + (1 - b)}
    cpeer = {"tp": 1 - core}
    znext = {"rep": znear}
    zmid = {"rep": last - z}
    outer = jnp.logical_or(z == 0, z == last)
    inner = jnp.logical_not(outer)
    token_peer = (apeer, bpeer)
    weight_peer = (bpeer, apeer)
    scale = 1.0 / math.sqrt(rows * lax.axis_size("rep") * lax.axis_size("fs"))
    count = len(PIECES)

    def remote(src, dst, ssem, rsem, peer):
        return pltpu.make_async_remote_copy(
            src_ref=src, dst_ref=dst, send_sem=ssem, recv_sem=rsem,
            device_id=peer, device_id_type=MESH)

    def cut(i, size):
        return pl.ds(pl.multiple_of(i * size, size), size)

    place = (b, a)
    mine = [cut(place[q], depth) for q in range(2)]
    theirs = [cut(1 - place[q], depth) for q in range(2)]
    far_block = lambda q, p: 2 * (1 - a) + p if q == 0 else 2 * p + 1 - b
    own_block = lambda q, p: 2 * a + p if q == 0 else 2 * p + b
    low = cut(core, part)
    mid = pl.ds(pl.multiple_of(rows + core * part, part), part)
    mid_other = pl.ds(pl.multiple_of(rows + (1 - core) * part, part), part)
    both = [(q, p) for q in range(2) for p in range(2)]
    halves = range(PARTS)

    def their_rows(q, h):
        return cut(PARTS * (1 - place[q]) + h, piece_rows)

    def piece_cols(k):
        j, first, units = PIECES[k]
        return j, pl.ds(first * unit, units * unit)

    def hp_cols(q, k):
        j, first, units = PIECES[k]
        return pl.ds(q * half + j * fc + first * unit, units * unit)

    def chunk(q, j):
        return q * STEPS + j

    def load_og(q, p):
        return pltpu.make_async_copy(
            og.at[:, cut(own_block(q, p), depth)],
            ogcat.at[q, pl.ds(0, rows), pl.ds(p * depth, depth)], l_og.at[q, p])

    def load_w(c):
        return pltpu.make_async_copy(
            w.at[:, pl.ds(c * fc, fc)], whalf.at[c, mine[c // STEPS]], l_w.at[c])

    def load_hp(c):
        return pltpu.make_async_copy(hp.at[:, pl.ds(c * fc, fc)], hpc.at[0, c], l_hp.at[c])

    def send_og(q, p):
        return remote(og.at[low, cut(far_block(q, p), depth)],
                      ogcat.at[q, mid, cut(p, depth)],
                      og_s.at[q, p], og_r.at[q, p], token_peer[q])

    def pass_og(q, p, span):
        spot = ogcat.at[q, span, cut(p, depth)]
        return remote(spot, spot, od_s.at[q, p], od_r.at[q, p], cpeer)

    def send_w(q, h):
        c = chunk(q, z)
        return remote(w.at[h * w_rows:(h + 1) * w_rows, cut(c, fc)],
                      whalf.at[c, cut(WPARTS * place[q] + h, w_rows)],
                      w_s.at[q, h], w_r.at[q, h], weight_peer[q])

    def pass_w(q, j, h, peer, ssem):
        c = chunk(q, j)
        spot = whalf.at[c, cut(WPARTS * (1 - place[q]) + h, w_rows)]
        return remote(spot, spot, ssem.at[c, h], f_r.at[c, h], peer)

    def near_w(q, j, h):
        return pass_w(q, j, h, znext, fn_s)

    def mid_w(q, j, h):
        return pass_w(q, j, h, zmid, fm_s)

    def send_hp(q, k):
        j, cols = piece_cols(k)
        return remote(hp.at[:, hp_cols(q, k)], hpc.at[1, chunk(q, j), :, cols],
                      hp_s.at[q, k], hp_r.at[q, k], token_peer[q])

    def send_pb(q, j):
        c = chunk(q, j)
        return remote(pbs.at[c], pbr.at[c], pb_s.at[c], pb_r.at[c], token_peer[q])

    def strip(ref, q, k, h):
        j, cols = piece_cols(k)
        return ref.at[chunk(q, j), pl.ds(h * piece_rows, piece_rows), cols]

    def send_g(q, k, h):
        return remote(strip(gs, q, k, h), strip(gr, q, k, h),
                      g_s.at[q, k, h], g_r.at[q, k, h], weight_peer[q])

    def send_z1(q, k, h):
        return remote(strip(zs, q, k, h), strip(z1r, q, k, h),
                      z1_s.at[q, k, h], z1_rs.at[q, k, h], znext)

    def send_z2(q, k, h):
        return remote(strip(zs, q, k, h), strip(z2r, q, k, h),
                      z2_s.at[q, k, h], z2_rs.at[q, k, h], zmid)

    def send_z3(q, k, h):
        return remote(strip(zt, q, k, h), strip(zt, q, k, h),
                      z3_s.at[q, k, h], z3_rs.at[q, k, h], znext)

    def act_of(q, k):
        j, cols = piece_cols(k)
        held = hpc[:, chunk(q, j), :, cols]
        positive = jnp.maximum(held.reshape(2 * rows, held.shape[-1]).astype(F32), 0.0)
        return (positive * positive).astype(BF)

    def g_out(q, k, act):
        for h in halves:
            strip(gs, q, k, h)[...] = jnp.dot(
                ogt[q, their_rows(q, h), :], act, preferred_element_type=F32).astype(BF)
            send_g(q, k, h).start()

    def g_own(q, k, act):
        j, cols = piece_cols(k)
        gown[chunk(q, j), :, cols] = jnp.dot(
            ogt[q, mine[q], :], act, preferred_element_type=F32)

    loaded = set()

    def once(name, copies):
        if name not in loaded:
            loaded.add(name)
            for copy in copies():
                copy.wait()

    def transpose_own(q):
        once("og", lambda: [load_og(*at) for at in both])
        ogt[q, :, 0:rows] = ogcat[q, 0:rows, :].T

    def og_part(q, far):
        return 1 - place[q] if far else place[q]

    def og_relay(q, far):
        p = og_part(q, far)
        send_og(q, p).wait_recv()
        pass_og(q, p, mid).start()

    def og_whole(q, far):
        p = og_part(q, far)
        pass_og(q, p, mid_other).wait_recv()
        ogt[q, cut(p, depth), rows:2 * rows] = ogcat[q, rows:2 * rows, cut(p, depth)].T

    def grad_send(q, k):
        c = chunk(q, PIECES[k][0])
        once(c, lambda: [load_hp(c)])
        send_hp(q, k).wait_recv()
        g_out(q, k, act_of(q, k))

    def grad_keep(q, k):
        g_own(q, k, act_of(q, k))

    def z_outer_send(q, k, h):
        send_g(q, k, h).wait_recv()
        strip(zs, q, k, h)[...] = (
            strip(gown, q, k, h)[...] + strip(gr, q, k, h)[...].astype(F32)).astype(BF)
        send_z1(q, k, h).start()

    def z_inner_send(q, k, h):
        send_g(q, k, h).wait_recv()
        send_z1(q, k, h).wait_recv()
        strip(zs, q, k, h)[...] = (
            strip(gown, q, k, h)[...] + strip(gr, q, k, h)[...].astype(F32)
            + strip(z1r, q, k, h)[...].astype(F32)).astype(BF)
        send_z2(q, k, h).start()

    def put_total(q, k, h, value):
        j, first, units = PIECES[k]
        tot_out[h * piece_rows:(h + 1) * piece_rows,
                q * half + j * fc + first * unit:q * half + j * fc + (first + units) * unit
                ] = value

    def z_inner_last(q, k, h):
        send_z2(q, k, h).wait_recv()
        value = (strip(zs, q, k, h)[...].astype(F32)
                 + strip(z2r, q, k, h)[...].astype(F32)).astype(BF)
        strip(zt, q, k, h)[...] = value
        send_z3(q, k, h).start()
        put_total(q, k, h, value)

    def z_outer_last(q, k, h):
        send_z3(q, k, h).wait_recv()
        put_total(q, k, h, strip(zt, q, k, h)[...])

    order = (z, znear, jnp.where(outer, last - znear, last - z), jnp.where(outer, last - z, last - znear))

    def w_own(q, h):
        send_w(q, h).wait_recv()
        near_w(q, z, h).start()

        @pl.when(inner)
        def _():
            mid_w(q, z, h).start()

    def w_down(q, h):
        mid_w(q, last - z, h).wait_recv()
        near_w(q, last - z, h).start()

    def w_across(q, h):
        near_w(q, znear, h).wait_recv()
        mid_w(q, znear, h).start()

    def w_far(q, h):
        mid_w(q, last - znear, h).wait_recv()
        near_w(q, last - znear, h).start()

    def back_send(q, i):
        once("w", lambda: [load_w(c) for c in range(2 * STEPS)])
        c = chunk(q, order[i])
        if i > 0:
            @pl.when(outer)
            def _():
                for h in range(WPARTS):
                    near_w(q, order[i], h).wait_recv()
        pbs[c] = jnp.dot(ogcat[q, rows:2 * rows, :], whalf[c], preferred_element_type=F32).astype(BF)
        send_pb(q, order[i]).start()

    def back_keep(q, i):
        c = chunk(q, order[i])
        pbo[c] = jnp.dot(ogcat[q, 0:rows, :], whalf[c], preferred_element_type=F32)

    def finish(q, i):
        c = chunk(q, order[i])
        send_pb(q, order[i]).wait_recv()
        positive = jnp.maximum(hpc[0, c].astype(F32), 0.0)
        hg_out[:, cut(c, fc)] = (2.0 * positive * (pbo[c] + pbr[c].astype(F32))).astype(BF)

    shared = {
        "sw": lambda q, h: send_w(q, h).start(),
        "sog": lambda q, far: send_og(q, og_part(q, far)).start(),
        "shp": lambda q, k: send_hp(q, k).start(),
        "tr0": transpose_own, "ogr": og_relay, "ogt": og_whole,
        "gout": grad_send, "gown": grad_keep, "w1": w_own,
        "bk": back_send, "bko": back_keep, "fin": finish,
    }
    at_outer = {"za": z_outer_send, "zd": z_outer_last}
    at_inner = {"zb": z_inner_send, "zc": z_inner_last, "w2a": w_down, "w2b": w_across, "w3": w_far}

    def run_group(table, role, group):
        steps = [(table[name], args) for name, *args in group if name in table]
        if steps:
            @pl.when(role)
            def _():
                for act, args in steps:
                    act(*args)

    barrier = pltpu.get_barrier_semaphore()
    for peer in (apeer, bpeer, cpeer, znext, zmid):
        pl.semaphore_signal(barrier, inc=1, device_id=peer, device_id_type=MESH)
    for q, p in both:
        load_og(q, p).start()
    pl.semaphore_wait(barrier, 5)
    group = []
    started = False
    for step in PLAN:
        if step[0] in shared:
            run_group(at_outer, outer, group)
            run_group(at_inner, inner, group)
            group = []
            if not started and step[0] == "tr0":
                started = True
                for c in range(2 * STEPS):
                    load_hp(c).start()
                for c in range(2 * STEPS):
                    load_w(c).start()
            shared[step[0]](*step[1:])
        else:
            group.append(step)
    run_group(at_outer, outer, group)
    run_group(at_inner, inner, group)

    for q, p in both:
        send_og(q, p).wait_send()
        pass_og(q, p, mid).wait_send()
    for q in range(2):
        for h in range(WPARTS):
            send_w(q, h).wait_send()
            near_w(q, z, h).wait_send()
        for k in range(count):
            send_hp(q, k).wait_send()
        for j in range(STEPS):
            send_pb(q, j).wait_send()
    pieces = [(q, k, h) for k in range(count) for q in range(2) for h in halves]
    for q, k, h in pieces:
        send_g(q, k, h).wait_send()

    @pl.when(outer)
    def _():
        for q, k, h in pieces:
            send_z1(q, k, h).wait_send()

    @pl.when(inner)
    def _():
        for q in range(2):
            for h in range(WPARTS):
                mid_w(q, z, h).wait_send()
                mid_w(q, znear, h).wait_send()
                near_w(q, last - z, h).wait_send()
                near_w(q, last - znear, h).wait_send()
        for q, k, h in pieces:
            send_z2(q, k, h).wait_send()
            send_z3(q, k, h).wait_send()


def put_kernel(hg, total, hg_out, tot_out, wide, sems):
    size = hg.shape[0] // PUTS
    tokens_all = size * PUTS * lax.axis_size("rep") * lax.axis_size("fs")
    copies = []
    for i in range(PUTS):
        span = pl.ds(i * size, size)
        copies.append(pltpu.make_async_copy(hg.at[span], hg_out.at[span], sems.at[1, i]))
        copies[-1].start()
        wide[span] = total[span].astype(F32) * (1.0 / math.sqrt(tokens_all))
        copies.append(pltpu.make_async_copy(wide.at[span], tot_out.at[span], sems.at[0, i]))
        copies[-1].start()
    for copy in copies:
        copy.wait()


def paired_body(hidden_pre, out_grad, down_weight):
    rows, ff = hidden_pre.shape
    depth = down_weight.shape[0]
    chunks = 2 * STEPS
    fc = ff // chunks
    count = len(PIECES)
    any_spec = pl.BlockSpec(memory_space=pl.ANY)
    vmem_spec = pl.BlockSpec(memory_space=pltpu.VMEM)

    def block(r, dtype):
        return pltpu.VMEM((chunks, r, fc), dtype)

    sem = pltpu.SemaphoreType.DMA
    hidden_grad, total = pl.pallas_call(
        kernel,
        out_shape=(jax.ShapeDtypeStruct((rows, ff), BF), jax.ShapeDtypeStruct((depth, ff), BF)),
        in_specs=[any_spec] * 3,
        out_specs=(vmem_spec, vmem_spec),
        scratch_shapes=[
            pltpu.VMEM((2, 2 * rows, 2 * depth), BF),
            pltpu.VMEM((2, 2 * depth, 2 * rows), BF),
            block(2 * depth, BF),
            pltpu.VMEM((2, chunks, rows, fc), BF),
            block(rows, BF), block(rows, BF), block(rows, F32),
            block(depth, BF), block(depth, BF), block(depth, F32),
            block(depth, BF), block(depth, BF), block(depth, BF), block(depth, BF),
            sem((2, 2)), sem((chunks,)), sem((chunks,)),
        ] + [sem((2, 2))] * 4 + [sem((2, WPARTS))] * 2 + [sem((chunks, WPARTS))] * 3 + [sem((chunks,))] * 2
        + [sem((2, count))] * 2 + [sem((2, count, PARTS))] * 8,
        compiler_params=pltpu.CompilerParams(
            collective_id=0, has_side_effects=True, vmem_limit_bytes=48 * 1024 * 1024
        ),
    )(hidden_pre, out_grad, down_weight)
    return pl.pallas_call(
        put_kernel,
        out_shape=(jax.ShapeDtypeStruct((rows, ff), BF), jax.ShapeDtypeStruct((depth, ff), F32)),
        in_specs=[any_spec, vmem_spec],
        out_specs=(any_spec, any_spec),
        scratch_shapes=[pltpu.VMEM((depth, ff), F32), pltpu.SemaphoreType.DMA((2, PUTS))],
        compiler_params=pltpu.CompilerParams(vmem_limit_bytes=8 * 1024 * 1024),
    )(hidden_grad, total)


def solution(mesh):
    placed = (P(("rep", "fs"), "tp"), P(("rep", "fs"), None), P("fs", "tp"))
    two_by_two = mesh.shape["fs"] == 4 and mesh.shape["tp"] == 2 and mesh.shape["rep"] == 4
    return jax.shard_map(
        paired_body if two_by_two else plain_body,
        mesh=mesh,
        in_specs=placed,
        out_specs=(P(("rep", "fs"), "tp"), P("fs", "tp")),
        check_vma=False,
    )
```

```python
import math

import jax
import jax.numpy as jnp
from jax import lax
from jax.experimental import pallas as pl
from jax.experimental.pallas import tpu as pltpu
from jax.sharding import PartitionSpec as P

MESH = pl.DeviceIdType.MESH
BF = jnp.bfloat16
F32 = jnp.float32


def plain_body(hidden_pre, out_grad, down_weight):
    rows = hidden_pre.shape[0]
    ff_local = hidden_pre.shape[1]
    back = jnp.dot(
        out_grad,
        lax.all_gather(down_weight, "fs", axis=0, tiled=True),
        preferred_element_type=F32,
    )
    positive = jnp.maximum(hidden_pre.astype(F32), 0.0)
    hidden_grad = (2.0 * positive * back).astype(BF)
    act = (positive * positive).astype(BF)
    partial_value = lax.dot_general(
        out_grad, act, (((0,), (0,)), ((), ())), preferred_element_type=F32
    )
    partial_value = partial_value.astype(BF)
    received = lax.all_to_all(partial_value, "fs", split_axis=0, concat_axis=0, tiled=True)
    groups = lax.axis_size("fs")
    local_sum = jnp.sum(
        received.reshape(groups, received.shape[0] // groups, ff_local), axis=0, dtype=F32
    )
    total = lax.psum(local_sum, "rep")
    tokens_all = rows * lax.axis_size("rep") * groups
    return (hidden_grad, total * (1.0 / math.sqrt(tokens_all)))


STEPS = 4
PIECES = ((0, 0, 2), (1, 0, 2), (2, 0, 2), (3, 0, 2))
PUTS = 4
PARTS = 2
WPARTS = 2
PLAN = (
    ("sw", 1, 1), ("sw", 1, 0), ("sw", 0, 0), ("sw", 0, 1), ("tr0", 0), ("sog", 1, 1), ("w1", 0, 0),
    ("sog", 0, 1), ("w1", 1, 0), ("w2b", 0, 0), ("sog", 1, 0), ("w1", 0, 1), ("shp", 0, 0), ("sog", 0, 0),
    ("w1", 1, 1), ("ogr", 0, 1), ("shp", 1, 3), ("ogr", 1, 1), ("ogt", 1, 1), ("ogt", 0, 1), ("w2b", 1, 0),
    ("w2a", 0, 0), ("tr0", 1), ("w2b", 1, 1), ("w2a", 0, 1), ("w2a", 1, 0), ("gout", 0, 0), ("w2b", 0, 1),
    ("shp", 0, 2), ("ogr", 1, 0), ("w2a", 1, 1), ("shp", 1, 2), ("w3", 0, 0), ("ogr", 0, 0), ("gout", 1, 3),
    ("ogt", 0, 0), ("w3", 1, 0), ("shp", 0, 1), ("gown", 0, 0), ("ogt", 1, 0), ("za", 0, 0, 0), ("w3", 1, 1),
    ("za", 0, 0, 1), ("gown", 1, 3), ("gout", 0, 2), ("shp", 1, 0), ("za", 1, 3, 0), ("zb", 0, 0, 0),
    ("gown", 0, 2), ("w3", 0, 1), ("za", 1, 3, 1), ("zb", 0, 0, 1), ("gout", 1, 2), ("zb", 1, 3, 0),
    ("za", 0, 2, 0), ("za", 0, 2, 1), ("zc", 0, 0, 0), ("zb", 1, 3, 1), ("zc", 0, 0, 1), ("gown", 1, 2),
    ("shp", 0, 3), ("zb", 0, 2, 0), ("zc", 1, 3, 0), ("za", 1, 2, 0), ("gout", 0, 1), ("za", 1, 2, 1),
    ("gown", 0, 1), ("shp", 1, 1), ("zb", 0, 2, 1), ("zc", 1, 3, 1), ("za", 0, 1, 0), ("gout", 1, 0),
    ("zb", 1, 2, 0), ("bk", 0, 3), ("zc", 0, 2, 0), ("za", 0, 1, 1), ("zb", 1, 2, 1), ("gown", 1, 0),
    ("zc", 0, 2, 1), ("zb", 0, 1, 0), ("zc", 1, 2, 0), ("gout", 0, 3), ("bk", 1, 2), ("zb", 0, 1, 1),
    ("za", 1, 0, 0), ("gown", 0, 3), ("zc", 1, 2, 1), ("za", 1, 0, 1), ("zb", 1, 0, 0), ("zd", 1, 3, 1),
    ("zc", 0, 1, 0), ("gout", 1, 1), ("zb", 1, 0, 1), ("za", 0, 3, 0), ("zd", 0, 2, 1), ("bk", 1, 1),
    ("zc", 0, 1, 1), ("gown", 1, 1), ("bk", 0, 1), ("zb", 0, 3, 0), ("za", 0, 3, 1), ("bko", 0, 1),
    ("zd", 1, 2, 1), ("zc", 1, 0, 0), ("zb", 0, 3, 1), ("za", 1, 1, 0), ("bk", 1, 0), ("zd", 0, 0, 0),
    ("zd", 1, 3, 0), ("za", 1, 1, 1), ("zc", 1, 0, 1), ("zb", 1, 1, 0), ("zc", 0, 3, 0), ("bk", 0, 2),
    ("bko", 0, 3), ("bko", 1, 2), ("zb", 1, 1, 1), ("zc", 0, 3, 1), ("bk", 1, 3), ("bko", 1, 1),
    ("bk", 0, 0), ("zc", 1, 1, 0), ("zd", 0, 2, 0), ("fin", 0, 1), ("bko", 1, 3), ("zd", 1, 2, 0),
    ("zd", 1, 0, 0), ("fin", 0, 3), ("bko", 1, 0), ("zc", 1, 1, 1), ("fin", 1, 2), ("zd", 1, 0, 1),
    ("bko", 0, 0), ("zd", 0, 1, 1), ("bko", 0, 2), ("zd", 0, 0, 1), ("zd", 0, 1, 0), ("zd", 0, 3, 1),
    ("zd", 1, 1, 0), ("fin", 0, 2), ("zd", 0, 3, 0), ("fin", 1, 1), ("fin", 1, 0), ("fin", 1, 3),
    ("fin", 0, 0), ("zd", 1, 1, 1),
)


def kernel(hp, og, w, hg_out, tot_out,
           ogcat, ogt, whalf, hpc, pbs, pbr, pbo, gs, gr, gown, zs, z1r, z2r, zt,
           l_og, l_w, l_hp,
           og_s, og_r, od_s, od_r, w_s, w_r, fn_s, fm_s, f_r, pb_s, pb_r,
           hp_s, hp_r, g_s, g_r, z1_s, z1_rs, z2_s, z2_rs, z3_s, z3_rs):
    rows, ff = hp.shape
    depth = w.shape[0]
    half = ff // 2
    fc = half // STEPS
    unit = fc // 2
    part = rows // 2
    w_rows = depth // WPARTS
    piece_rows = depth // PARTS
    fs = lax.axis_index("fs")
    core = lax.axis_index("tp")
    z = lax.axis_index("rep")
    last = lax.axis_size("rep") - 1
    a, b = fs // 2, fs % 2
    znear = z + 1 - 2 * (z % 2)
    apeer = {"fs": (1 - a) * 2 + b}
    bpeer = {"fs": a * 2 + (1 - b)}
    cpeer = {"tp": 1 - core}
    znext = {"rep": znear}
    zmid = {"rep": last - z}
    outer = jnp.logical_or(z == 0, z == last)
    inner = jnp.logical_not(outer)
    token_peer = (apeer, bpeer)
    weight_peer = (bpeer, apeer)
    scale = 1.0 / math.sqrt(rows * lax.axis_size("rep") * lax.axis_size("fs"))
    count = len(PIECES)

    def remote(src, dst, ssem, rsem, peer):
        return pltpu.make_async_remote_copy(
            src_ref=src, dst_ref=dst, send_sem=ssem, recv_sem=rsem,
            device_id=peer, device_id_type=MESH)

    def cut(i, size):
        return pl.ds(pl.multiple_of(i * size, size), size)

    place = (b, a)
    mine = [cut(place[q], depth) for q in range(2)]
    theirs = [cut(1 - place[q], depth) for q in range(2)]
    far_block = lambda q, p: 2 * (1 - a) + p if q == 0 else 2 * p + 1 - b
    own_block = lambda q, p: 2 * a + p if q == 0 else 2 * p + b
    low = cut(core, part)
    mid = pl.ds(pl.multiple_of(rows + core * part, part), part)
    mid_other = pl.ds(pl.multiple_of(rows + (1 - core) * part, part), part)
    both = [(q, p) for q in range(2) for p in range(2)]
    halves = range(PARTS)

    def their_rows(q, h):
        return cut(PARTS * (1 - place[q]) + h, piece_rows)

    def piece_cols(k):
        j, first, units = PIECES[k]
        return j, pl.ds(first * unit, units * unit)

    def hp_cols(q, k):
        j, first, units = PIECES[k]
        return pl.ds(q * half + j * fc + first * unit, units * unit)

    def chunk(q, j):
        return q * STEPS + j

    def load_og(q, p):
        return pltpu.make_async_copy(
            og.at[:, cut(own_block(q, p), depth)],
            ogcat.at[q, pl.ds(0, rows), pl.ds(p * depth, depth)], l_og.at[q, p])

    def load_w(c):
        return pltpu.make_async_copy(
            w.at[:, pl.ds(c * fc, fc)], whalf.at[c, mine[c // STEPS]], l_w.at[c])

    def load_hp(c):
        return pltpu.make_async_copy(hp.at[:, pl.ds(c * fc, fc)], hpc.at[0, c], l_hp.at[c])

    def send_og(q, p):
        return remote(og.at[low, cut(far_block(q, p), depth)],
                      ogcat.at[q, mid, cut(p, depth)],
                      og_s.at[q, p], og_r.at[q, p], token_peer[q])

    def pass_og(q, p, span):
        spot = ogcat.at[q, span, cut(p, depth)]
        return remote(spot, spot, od_s.at[q, p], od_r.at[q, p], cpeer)

    def send_w(q, h):
        c = chunk(q, z)
        return remote(w.at[h * w_rows:(h + 1) * w_rows, cut(c, fc)],
                      whalf.at[c, cut(WPARTS * place[q] + h, w_rows)],
                      w_s.at[q, h], w_r.at[q, h], weight_peer[q])

    def pass_w(q, j, h, peer, ssem):
        c = chunk(q, j)
        spot = whalf.at[c, cut(WPARTS * (1 - place[q]) + h, w_rows)]
        return remote(spot, spot, ssem.at[c, h], f_r.at[c, h], peer)

    def near_w(q, j, h):
        return pass_w(q, j, h, znext, fn_s)

    def mid_w(q, j, h):
        return pass_w(q, j, h, zmid, fm_s)

    def send_hp(q, k):
        j, cols = piece_cols(k)
        return remote(hp.at[:, hp_cols(q, k)], hpc.at[1, chunk(q, j), :, cols],
                      hp_s.at[q, k], hp_r.at[q, k], token_peer[q])

    def send_pb(q, j):
        c = chunk(q, j)
        return remote(pbs.at[c], pbr.at[c], pb_s.at[c], pb_r.at[c], token_peer[q])

    def strip(ref, q, k, h):
        j, cols = piece_cols(k)
        return ref.at[chunk(q, j), pl.ds(h * piece_rows, piece_rows), cols]

    def send_g(q, k, h):
        return remote(strip(gs, q, k, h), strip(gr, q, k, h),
                      g_s.at[q, k, h], g_r.at[q, k, h], weight_peer[q])

    def send_z1(q, k, h):
        return remote(strip(zs, q, k, h), strip(z1r, q, k, h),
                      z1_s.at[q, k, h], z1_rs.at[q, k, h], znext)

    def send_z2(q, k, h):
        return remote(strip(zs, q, k, h), strip(z2r, q, k, h),
                      z2_s.at[q, k, h], z2_rs.at[q, k, h], zmid)

    def send_z3(q, k, h):
        return remote(strip(zt, q, k, h), strip(zt, q, k, h),
                      z3_s.at[q, k, h], z3_rs.at[q, k, h], znext)

    def act_of(q, k):
        j, cols = piece_cols(k)
        held = hpc[:, chunk(q, j), :, cols]
        positive = jnp.maximum(held.reshape(2 * rows, held.shape[-1]).astype(F32), 0.0)
        return (positive * positive).astype(BF)

    def g_out(q, k, act):
        for h in halves:
            strip(gs, q, k, h)[...] = jnp.dot(
                ogt[q, their_rows(q, h), :], act, preferred_element_type=F32).astype(BF)
            send_g(q, k, h).start()

    def g_own(q, k, act):
        j, cols = piece_cols(k)
        gown[chunk(q, j), :, cols] = jnp.dot(
            ogt[q, mine[q], :], act, preferred_element_type=F32)

    loaded = set()

    def once(name, copies):
        if name not in loaded:
            loaded.add(name)
            for copy in copies():
                copy.wait()

    def transpose_own(q):
        once("og", lambda: [load_og(*at) for at in both])
        ogt[q, :, 0:rows] = ogcat[q, 0:rows, :].T

    def og_part(q, far):
        return 1 - place[q] if far else place[q]

    def og_relay(q, far):
        p = og_part(q, far)
        send_og(q, p).wait_recv()
        pass_og(q, p, mid).start()

    def og_whole(q, far):
        p = og_part(q, far)
        pass_og(q, p, mid_other).wait_recv()
        ogt[q, cut(p, depth), rows:2 * rows] = ogcat[q, rows:2 * rows, cut(p, depth)].T

    def grad_send(q, k):
        c = chunk(q, PIECES[k][0])
        once(c, lambda: [load_hp(c)])
        send_hp(q, k).wait_recv()
        g_out(q, k, act_of(q, k))

    def grad_keep(q, k):
        g_own(q, k, act_of(q, k))

    def z_outer_send(q, k, h):
        send_g(q, k, h).wait_recv()
        strip(zs, q, k, h)[...] = (
            strip(gown, q, k, h)[...] + strip(gr, q, k, h)[...].astype(F32)).astype(BF)
        send_z1(q, k, h).start()

    def z_inner_send(q, k, h):
        send_g(q, k, h).wait_recv()
        send_z1(q, k, h).wait_recv()
        strip(zs, q, k, h)[...] = (
            strip(gown, q, k, h)[...] + strip(gr, q, k, h)[...].astype(F32)
            + strip(z1r, q, k, h)[...].astype(F32)).astype(BF)
        send_z2(q, k, h).start()

    def put_total(q, k, h, value):
        j, first, units = PIECES[k]
        tot_out[h * piece_rows:(h + 1) * piece_rows,
                q * half + j * fc + first * unit:q * half + j * fc + (first + units) * unit
                ] = value

    def z_inner_last(q, k, h):
        send_z2(q, k, h).wait_recv()
        value = (strip(zs, q, k, h)[...].astype(F32)
                 + strip(z2r, q, k, h)[...].astype(F32)).astype(BF)
        strip(zt, q, k, h)[...] = value
        send_z3(q, k, h).start()
        put_total(q, k, h, value)

    def z_outer_last(q, k, h):
        send_z3(q, k, h).wait_recv()
        put_total(q, k, h, strip(zt, q, k, h)[...])

    order = (z, znear, jnp.where(outer, last - znear, last - z), jnp.where(outer, last - z, last - znear))

    def w_own(q, h):
        send_w(q, h).wait_recv()
        near_w(q, z, h).start()

        @pl.when(inner)
        def _():
            mid_w(q, z, h).start()

    def w_down(q, h):
        mid_w(q, last - z, h).wait_recv()
        near_w(q, last - z, h).start()

    def w_across(q, h):
        near_w(q, znear, h).wait_recv()
        mid_w(q, znear, h).start()

    def w_far(q, h):
        mid_w(q, last - znear, h).wait_recv()
        near_w(q, last - znear, h).start()

    def back_send(q, i):
        once("w", lambda: [load_w(c) for c in range(2 * STEPS)])
        c = chunk(q, order[i])
        if i > 0:
            @pl.when(outer)
            def _():
                for h in range(WPARTS):
                    near_w(q, order[i], h).wait_recv()
        pbs[c] = jnp.dot(ogcat[q, rows:2 * rows, :], whalf[c], preferred_element_type=F32).astype(BF)
        send_pb(q, order[i]).start()

    def back_keep(q, i):
        c = chunk(q, order[i])
        pbo[c] = jnp.dot(ogcat[q, 0:rows, :], whalf[c], preferred_element_type=F32)

    def finish(q, i):
        c = chunk(q, order[i])
        send_pb(q, order[i]).wait_recv()
        positive = jnp.maximum(hpc[0, c].astype(F32), 0.0)
        hg_out[:, cut(c, fc)] = (2.0 * positive * (pbo[c] + pbr[c].astype(F32))).astype(BF)

    shared = {
        "sw": lambda q, h: send_w(q, h).start(),
        "sog": lambda q, far: send_og(q, og_part(q, far)).start(),
        "shp": lambda q, k: send_hp(q, k).start(),
        "tr0": transpose_own, "ogr": og_relay, "ogt": og_whole,
        "gout": grad_send, "gown": grad_keep, "w1": w_own,
        "bk": back_send, "bko": back_keep, "fin": finish,
    }
    at_outer = {"za": z_outer_send, "zd": z_outer_last}
    at_inner = {"zb": z_inner_send, "zc": z_inner_last, "w2a": w_down, "w2b": w_across, "w3": w_far}

    def run_group(table, role, group):
        steps = [(table[name], args) for name, *args in group if name in table]
        if steps:
            @pl.when(role)
            def _():
                for act, args in steps:
                    act(*args)

    barrier = pltpu.get_barrier_semaphore()
    for peer in (apeer, bpeer, cpeer, znext):
        pl.semaphore_signal(barrier, inc=1, device_id=peer, device_id_type=MESH)

    @pl.when(inner)
    def _():
        pl.semaphore_signal(barrier, inc=1, device_id=zmid, device_id_type=MESH)

    for q, p in both:
        load_og(q, p).start()
    pl.semaphore_wait(barrier, jnp.where(outer, 4, 5))
    group = []
    started = False
    for step in PLAN:
        if step[0] in shared:
            run_group(at_outer, outer, group)
            run_group(at_inner, inner, group)
            group = []
            if not started and step[0] == "tr0":
                started = True
                for c in range(2 * STEPS):
                    load_hp(c).start()
                for c in range(2 * STEPS):
                    load_w(c).start()
            shared[step[0]](*step[1:])
        else:
            group.append(step)
    run_group(at_outer, outer, group)
    run_group(at_inner, inner, group)

    for q, p in both:
        send_og(q, p).wait_send()
        pass_og(q, p, mid).wait_send()
    for q in range(2):
        for h in range(WPARTS):
            send_w(q, h).wait_send()
            near_w(q, z, h).wait_send()
        for k in range(count):
            send_hp(q, k).wait_send()
        for j in range(STEPS):
            send_pb(q, j).wait_send()
    pieces = [(q, k, h) for k in range(count) for q in range(2) for h in halves]
    for q, k, h in pieces:
        send_g(q, k, h).wait_send()

    @pl.when(outer)
    def _():
        for q, k, h in pieces:
            send_z1(q, k, h).wait_send()

    @pl.when(inner)
    def _():
        for q in range(2):
            for h in range(WPARTS):
                mid_w(q, z, h).wait_send()
                mid_w(q, znear, h).wait_send()
                near_w(q, last - z, h).wait_send()
                near_w(q, last - znear, h).wait_send()
        for q, k, h in pieces:
            send_z2(q, k, h).wait_send()
            send_z3(q, k, h).wait_send()


def put_kernel(hg, total, hg_out, tot_out, wide, sems):
    size = hg.shape[0] // PUTS
    tokens_all = size * PUTS * lax.axis_size("rep") * lax.axis_size("fs")
    copies = []
    for i in range(PUTS):
        span = pl.ds(i * size, size)
        copies.append(pltpu.make_async_copy(hg.at[span], hg_out.at[span], sems.at[1, i]))
        copies[-1].start()
        wide[span] = total[span].astype(F32) * (1.0 / math.sqrt(tokens_all))
        copies.append(pltpu.make_async_copy(wide.at[span], tot_out.at[span], sems.at[0, i]))
        copies[-1].start()
    for copy in copies:
        copy.wait()


def paired_body(hidden_pre, out_grad, down_weight):
    rows, ff = hidden_pre.shape
    depth = down_weight.shape[0]
    chunks = 2 * STEPS
    fc = ff // chunks
    count = len(PIECES)
    any_spec = pl.BlockSpec(memory_space=pl.ANY)
    vmem_spec = pl.BlockSpec(memory_space=pltpu.VMEM)

    def block(r, dtype):
        return pltpu.VMEM((chunks, r, fc), dtype)

    sem = pltpu.SemaphoreType.DMA
    hidden_grad, total = pl.pallas_call(
        kernel,
        out_shape=(jax.ShapeDtypeStruct((rows, ff), BF), jax.ShapeDtypeStruct((depth, ff), BF)),
        in_specs=[any_spec] * 3,
        out_specs=(vmem_spec, vmem_spec),
        scratch_shapes=[
            pltpu.VMEM((2, 2 * rows, 2 * depth), BF),
            pltpu.VMEM((2, 2 * depth, 2 * rows), BF),
            block(2 * depth, BF),
            pltpu.VMEM((2, chunks, rows, fc), BF),
            block(rows, BF), block(rows, BF), block(rows, F32),
            block(depth, BF), block(depth, BF), block(depth, F32),
            block(depth, BF), block(depth, BF), block(depth, BF), block(depth, BF),
            sem((2, 2)), sem((chunks,)), sem((chunks,)),
        ] + [sem((2, 2))] * 4 + [sem((2, WPARTS))] * 2 + [sem((chunks, WPARTS))] * 3 + [sem((chunks,))] * 2
        + [sem((2, count))] * 2 + [sem((2, count, PARTS))] * 8,
        compiler_params=pltpu.CompilerParams(
            collective_id=0, has_side_effects=True, vmem_limit_bytes=48 * 1024 * 1024
        ),
    )(hidden_pre, out_grad, down_weight)
    return pl.pallas_call(
        put_kernel,
        out_shape=(jax.ShapeDtypeStruct((rows, ff), BF), jax.ShapeDtypeStruct((depth, ff), F32)),
        in_specs=[any_spec, vmem_spec],
        out_specs=(any_spec, any_spec),
        scratch_shapes=[pltpu.VMEM((depth, ff), F32), pltpu.SemaphoreType.DMA((2, PUTS))],
        compiler_params=pltpu.CompilerParams(vmem_limit_bytes=8 * 1024 * 1024),
    )(hidden_grad, total)


def solution(mesh):
    placed = (P(("rep", "fs"), "tp"), P(("rep", "fs"), None), P("fs", "tp"))
    two_by_two = mesh.shape["fs"] == 4 and mesh.shape["tp"] == 2 and mesh.shape["rep"] == 4
    return jax.shard_map(
        paired_body if two_by_two else plain_body,
        mesh=mesh,
        in_specs=placed,
        out_specs=(P(("rep", "fs"), "tp"), P("fs", "tp")),
        check_vma=False,
    )
```

```python
import math

import jax
import jax.numpy as jnp
from jax import lax
from jax.experimental import pallas as pl
from jax.experimental.pallas import tpu as pltpu
from jax.sharding import PartitionSpec as P

MESH = pl.DeviceIdType.MESH
BF = jnp.bfloat16
F32 = jnp.float32


def plain_body(hidden_pre, out_grad, down_weight):
    rows = hidden_pre.shape[0]
    ff_local = hidden_pre.shape[1]
    back = jnp.dot(
        out_grad,
        lax.all_gather(down_weight, "fs", axis=0, tiled=True),
        preferred_element_type=F32,
    )
    positive = jnp.maximum(hidden_pre.astype(F32), 0.0)
    hidden_grad = (2.0 * positive * back).astype(BF)
    act = (positive * positive).astype(BF)
    partial_value = lax.dot_general(
        out_grad, act, (((0,), (0,)), ((), ())), preferred_element_type=F32
    )
    partial_value = partial_value.astype(BF)
    received = lax.all_to_all(partial_value, "fs", split_axis=0, concat_axis=0, tiled=True)
    groups = lax.axis_size("fs")
    local_sum = jnp.sum(
        received.reshape(groups, received.shape[0] // groups, ff_local), axis=0, dtype=F32
    )
    total = lax.psum(local_sum, "rep")
    tokens_all = rows * lax.axis_size("rep") * groups
    return (hidden_grad, total * (1.0 / math.sqrt(tokens_all)))


STEPS = 4
PIECES = ((0, 0, 2), (1, 0, 1), (1, 1, 1), (2, 0, 2), (3, 0, 2))
SHIFT = 16
PUTS = 2
PARTS = 2
VIA_Z = 1
PLAN = (
    ("sw2", 1), ("sw1", 0), ("sw1", 1), ("sw", 0), ("w1c", 1), ("tr0", 0), ("sog", 1, 1), ("sw", 1),
    ("tr0", 1), ("w1b", 0), ("w1b", 1), ("sog", 0, 1), ("w1", 1), ("shp", 0, 1), ("w1", 0), ("sw2", 0),
    ("w4", 1), ("sog", 0, 0), ("shp", 1, 1), ("sog", 1, 0), ("w2b", 0, 1), ("ogr", 1, 1), ("w1c", 0),
    ("w2b", 1, 1), ("w2a", 1, 1), ("shp", 1, 2), ("ogr", 0, 1), ("w2a", 1, 0), ("ogt", 1, 1), ("shp", 0, 3),
    ("gout", 1, 1), ("ogt", 0, 1), ("shp", 1, 0), ("w2a", 0, 0), ("w3", 0, 1), ("w2b", 0, 0), ("w2b", 1, 0),
    ("w2a", 0, 1), ("zg", 1, 1, 0), ("gout", 0, 1), ("ogr", 1, 0), ("ogr", 0, 0), ("ogt", 1, 0),
    ("ogt", 0, 0), ("gown", 0, 1), ("gown", 1, 1), ("zg", 1, 1, 1), ("za", 1, 1, 0), ("za", 0, 1, 1),
    ("w3", 0, 0), ("gout", 1, 2), ("shp", 0, 2), ("zg", 0, 1, 0), ("za", 1, 1, 1), ("zg", 0, 1, 1),
    ("za", 0, 1, 0), ("w4", 0), ("gout", 0, 3), ("w3", 1, 0), ("w2a", 1, 2), ("zb", 1, 1, 0), ("gown", 1, 2),
    ("za", 1, 2, 1), ("gout", 1, 0), ("za", 1, 2, 0), ("w2a", 0, 2), ("gown", 0, 3), ("zb", 0, 1, 1),
    ("zc", 1, 1, 0), ("w3", 1, 1), ("zb", 1, 1, 1), ("shp", 1, 4), ("za", 0, 3, 0), ("zb", 1, 2, 1),
    ("zb", 1, 2, 0), ("gown", 1, 0), ("shp", 0, 4), ("gout", 0, 2), ("gown", 0, 2), ("zc", 1, 1, 1),
    ("zb", 0, 1, 0), ("zb", 0, 3, 0), ("za", 0, 3, 1), ("zc", 0, 1, 1), ("za", 1, 0, 0), ("zc", 1, 2, 1),
    ("shp", 1, 3), ("zc", 0, 1, 0), ("zb", 0, 3, 1), ("za", 1, 0, 1), ("gout", 1, 4), ("zc", 1, 2, 0),
    ("za", 0, 2, 0), ("shp", 0, 0), ("zc", 0, 3, 0), ("zb", 1, 0, 0), ("zb", 1, 0, 1), ("gout", 0, 4),
    ("zc", 0, 3, 1), ("zb", 0, 2, 0), ("zc", 1, 0, 0), ("zb", 0, 2, 1), ("za", 0, 2, 1), ("gown", 0, 4),
    ("gown", 1, 4), ("za", 1, 4, 0), ("bk", 1, 0), ("zd", 1, 1, 1), ("zc", 1, 0, 1), ("zb", 1, 4, 0),
    ("za", 1, 4, 1), ("gout", 1, 3), ("zc", 0, 2, 0), ("bk", 0, 3), ("zd", 1, 2, 0), ("bk", 0, 0),
    ("za", 0, 4, 0), ("zc", 0, 2, 1), ("bk", 0, 1), ("zb", 1, 4, 1), ("zd", 0, 1, 0), ("bko", 1, 0),
    ("gown", 1, 3), ("za", 0, 4, 1), ("zd", 1, 2, 1), ("zc", 1, 4, 0), ("gout", 0, 0), ("zb", 0, 4, 0),
    ("bko", 0, 3), ("bk", 1, 1), ("za", 1, 3, 0), ("zc", 1, 4, 1), ("zb", 0, 4, 1), ("gown", 0, 0),
    ("bk", 0, 2), ("za", 1, 3, 1), ("zb", 1, 3, 0), ("zd", 0, 3, 1), ("bko", 0, 0), ("zc", 0, 4, 0),
    ("bko", 1, 1), ("zc", 0, 4, 1), ("zb", 1, 3, 1), ("za", 0, 0, 0), ("zd", 1, 0, 1), ("zb", 0, 0, 0),
    ("bk", 1, 3), ("zd", 1, 4, 0), ("bk", 1, 2), ("za", 0, 0, 1), ("zd", 1, 1, 0), ("zc", 1, 3, 0),
    ("zc", 1, 3, 1), ("zb", 0, 0, 1), ("bko", 0, 1), ("zd", 0, 2, 0), ("zd", 0, 4, 1), ("zc", 0, 0, 0),
    ("zd", 1, 4, 1), ("bko", 1, 3), ("zc", 0, 0, 1), ("zd", 0, 3, 0), ("fin", 1, 3), ("fin", 0, 3),
    ("zd", 1, 3, 0), ("fin", 1, 0), ("zd", 1, 0, 0), ("zd", 0, 1, 1), ("fin", 0, 1), ("zd", 1, 3, 1),
    ("zd", 0, 2, 1), ("fin", 0, 0), ("bko", 1, 2), ("zd", 0, 0, 0), ("fin", 1, 1), ("zd", 0, 4, 0),
    ("bko", 0, 2), ("fin", 1, 2), ("fin", 0, 2), ("zd", 0, 0, 1),
)


def kernel(hp, og, w, hg_out, tot_out,
           ogcat, ogt, whalf, hpc, pbs, pbr, pbo, gs, gr, gown, zs, z1r, z2r, zt, wide, zgr,
           l_og, l_w, l_hp,
           og_s, og_r, od_s, od_r, w_s, w_r, fn_s, fm_s, f_r, pb_s, pb_r,
           hp_s, hp_r, g_s, g_r, z1_s, z1_rs, z2_s, z2_rs, z3_s, z3_rs, zg_s, zg_r):
    rows, ff = hp.shape
    depth = w.shape[0]
    half = ff // 2
    fc = half // STEPS
    unit = fc // 2
    part = rows // 2
    quarter = depth // 4
    outer_rows = ((0, 2), (2, 2))
    inner_rows = ((0, 2), (2, 1), (3, 1))
    piece_rows = depth // PARTS
    fs = lax.axis_index("fs")
    core = lax.axis_index("tp")
    z = lax.axis_index("rep")
    last = lax.axis_size("rep") - 1
    a, b = fs // 2, fs % 2
    znear = z + 1 - 2 * (z % 2)
    apeer = {"fs": (1 - a) * 2 + b}
    bpeer = {"fs": a * 2 + (1 - b)}
    cpeer = {"tp": 1 - core}
    znext = {"rep": znear}
    zmid = {"rep": last - z}
    outer = jnp.logical_or(z == 0, z == last)
    inner = jnp.logical_not(outer)
    token_peer = (apeer, bpeer)
    weight_peer = (bpeer, apeer)
    scale = 1.0 / math.sqrt(rows * lax.axis_size("rep") * lax.axis_size("fs"))
    count = len(PIECES)

    def remote(src, dst, ssem, rsem, peer):
        return pltpu.make_async_remote_copy(
            src_ref=src, dst_ref=dst, send_sem=ssem, recv_sem=rsem,
            device_id=peer, device_id_type=MESH)

    def cut(i, size):
        return pl.ds(pl.multiple_of(i * size, size), size)

    place = (b, a)
    mine = [cut(place[q], depth) for q in range(2)]
    theirs = [cut(1 - place[q], depth) for q in range(2)]
    far_block = lambda q, p: 2 * (1 - a) + p if q == 0 else 2 * p + 1 - b
    own_block = lambda q, p: 2 * a + p if q == 0 else 2 * p + b
    spans = ((0, part - rows // SHIFT), (part - rows // SHIFT, part + rows // SHIFT))
    both = [(q, p) for q in range(2) for p in range(2)]
    halves = range(PARTS)

    def their_rows(q, h):
        return cut(PARTS * (1 - place[q]) + h, piece_rows)

    def piece_cols(k):
        j, first, units = PIECES[k]
        return j, pl.ds(first * unit, units * unit)

    def hp_cols(q, k):
        j, first, units = PIECES[k]
        return pl.ds(q * half + j * fc + first * unit, units * unit)

    def chunk(q, j):
        return q * STEPS + j

    def load_og(q, p):
        return pltpu.make_async_copy(
            og.at[:, cut(own_block(q, p), depth)],
            ogcat.at[q, pl.ds(0, rows), pl.ds(p * depth, depth)], l_og.at[q, p])

    def load_w(c):
        return pltpu.make_async_copy(
            w.at[:, pl.ds(c * fc, fc)], whalf.at[c, mine[c // STEPS]], l_w.at[c])

    def load_hp(c):
        return pltpu.make_async_copy(hp.at[:, pl.ds(c * fc, fc)], hpc.at[0, c], l_hp.at[c])

    def on_core(step):
        for v in range(2):
            @pl.when(core == v)
            def _():
                step(v)

    def send_og(q, p, v):
        first, size = spans[v]
        return remote(og.at[pl.ds(first, size), cut(far_block(q, p), depth)],
                      ogcat.at[q, pl.ds(rows + first, size), cut(p, depth)],
                      og_s.at[q, p], og_r.at[q, p], token_peer[q])

    def pass_og(q, p, v):
        first, size = spans[v]
        spot = ogcat.at[q, pl.ds(rows + first, size), cut(p, depth)]
        return remote(spot, spot, od_s.at[q, p], od_r.at[q, p], cpeer)

    def fetch_w(q, j, part, slot):
        first, size = part
        c = chunk(q, j)
        rows_there = pl.ds(pl.multiple_of(place[q] * depth + first * quarter, quarter), size * quarter)
        return remote(w.at[pl.ds(first * quarter, size * quarter), cut(c, fc)],
                      whalf.at[c, rows_there], w_s.at[q, slot], w_r.at[q, slot], weight_peer[q])

    def pass_w(q, j, part, slot, peer, ssem):
        first, size = part
        c = chunk(q, j)
        spot = whalf.at[c, pl.ds(
            pl.multiple_of((1 - place[q]) * depth + first * quarter, quarter), size * quarter)]
        return remote(spot, spot, ssem.at[c, slot], f_r.at[c, slot], peer)

    def near_w(q, j, parts, h):
        return pass_w(q, j, parts[h], h, znext, fn_s)

    def mid_w(q, j, parts, h):
        return pass_w(q, j, parts[h], h, zmid, fm_s)

    def send_hp(q, k):
        j, cols = piece_cols(k)
        return remote(hp.at[:, hp_cols(q, k)], hpc.at[1, chunk(q, j), :, cols],
                      hp_s.at[q, k], hp_r.at[q, k], token_peer[q])

    def send_pb(q, j):
        c = chunk(q, j)
        return remote(pbs.at[c], pbr.at[c], pb_s.at[c], pb_r.at[c], token_peer[q])

    def strip(ref, q, k, h):
        j, cols = piece_cols(k)
        return ref.at[chunk(q, j), pl.ds(h * piece_rows, piece_rows), cols]

    def send_g(q, k, h):
        return remote(strip(gs, q, k, h), strip(gr, q, k, h),
                      g_s.at[q, k, h], g_r.at[q, k, h], weight_peer[q])

    def send_zg(q, h):
        return remote(strip(gs, q, VIA_Z, h), zgr.at[q, pl.ds(h * piece_rows, piece_rows)],
                      zg_s.at[q, h], zg_r.at[q, h], znext)

    def send_z1(q, k, h):
        return remote(strip(zs, q, k, h), strip(z1r, q, k, h),
                      z1_s.at[q, k, h], z1_rs.at[q, k, h], znext)

    def send_z2(q, k, h):
        return remote(strip(zs, q, k, h), strip(z2r, q, k, h),
                      z2_s.at[q, k, h], z2_rs.at[q, k, h], zmid)

    def send_z3(q, k, h):
        return remote(strip(zt, q, k, h), strip(zt, q, k, h),
                      z3_s.at[q, k, h], z3_rs.at[q, k, h], znext)

    def act_of(q, k):
        j, cols = piece_cols(k)
        held = hpc[:, chunk(q, j), :, cols]
        positive = jnp.maximum(held.reshape(2 * rows, held.shape[-1]).astype(F32), 0.0)
        return (positive * positive).astype(BF)

    def g_out(q, k, act):
        for h in halves:
            value = jnp.dot(ogt[q, their_rows(q, h), :], act, preferred_element_type=F32)
            if k == VIA_Z:
                wide[q, h * piece_rows:(h + 1) * piece_rows] = value

                @pl.when(outer)
                def _():
                    strip(gs, q, k, h)[...] = wide[q, h * piece_rows:(h + 1) * piece_rows].astype(BF)
                    send_zg(q, h).start()
            else:
                strip(gs, q, k, h)[...] = value.astype(BF)
                send_g(q, k, h).start()

    def g_own(q, k, act):
        j, cols = piece_cols(k)
        gown[chunk(q, j), :, cols] = jnp.dot(
            ogt[q, mine[q], :], act, preferred_element_type=F32)

    loaded = set()

    def once(name, copies):
        if name not in loaded:
            loaded.add(name)
            for copy in copies():
                copy.wait()

    def transpose_own(q):
        once("og", lambda: [load_og(*at) for at in both])
        ogt[q, :, 0:rows] = ogcat[q, 0:rows, :].T

    def og_part(q, far):
        return 1 - place[q] if far else place[q]

    def og_relay(q, far):
        p = og_part(q, far)

        def step(v):
            send_og(q, p, v).wait_recv()
            pass_og(q, p, v).start()

        on_core(step)

    def og_whole(q, far):
        p = og_part(q, far)
        on_core(lambda v: pass_og(q, p, 1 - v).wait_recv())
        ogt[q, cut(p, depth), rows:2 * rows] = ogcat[q, rows:2 * rows, cut(p, depth)].T

    def grad_send(q, k):
        c = chunk(q, PIECES[k][0])
        once(c, lambda: [load_hp(c)])
        send_hp(q, k).wait_recv()
        g_out(q, k, act_of(q, k))

    def grad_keep(q, k):
        g_own(q, k, act_of(q, k))

    def grad_merge(q, k, h):
        send_zg(q, h).wait_recv()
        strip(gs, q, k, h)[...] = (
            wide[q, h * piece_rows:(h + 1) * piece_rows]
            + zgr[q, h * piece_rows:(h + 1) * piece_rows].astype(F32)).astype(BF)
        send_g(q, k, h).start()

    def z_outer_send(q, k, h):
        value = strip(gown, q, k, h)[...]
        if k != VIA_Z:
            send_g(q, k, h).wait_recv()
            value = value + strip(gr, q, k, h)[...].astype(F32)
        strip(zs, q, k, h)[...] = value.astype(BF)
        send_z1(q, k, h).start()

    def z_inner_send(q, k, h):
        send_g(q, k, h).wait_recv()
        send_z1(q, k, h).wait_recv()
        strip(zs, q, k, h)[...] = (
            strip(gown, q, k, h)[...] + strip(gr, q, k, h)[...].astype(F32)
            + strip(z1r, q, k, h)[...].astype(F32)).astype(BF)
        send_z2(q, k, h).start()

    def put_total(q, k, h, value):
        j, first, units = PIECES[k]
        tot_out[h * piece_rows:(h + 1) * piece_rows,
                q * half + j * fc + first * unit:q * half + j * fc + (first + units) * unit
                ] = value

    def z_inner_last(q, k, h):
        send_z2(q, k, h).wait_recv()
        value = (strip(zs, q, k, h)[...].astype(F32)
                 + strip(z2r, q, k, h)[...].astype(F32)).astype(BF)
        strip(zt, q, k, h)[...] = value
        send_z3(q, k, h).start()
        put_total(q, k, h, value)

    def z_outer_last(q, k, h):
        send_z3(q, k, h).wait_recv()
        put_total(q, k, h, strip(zt, q, k, h)[...])

    order = (z, znear, jnp.where(outer, last - znear, last - z), jnp.where(outer, last - z, last - znear))

    def w_own(q):
        fetch_w(q, z, outer_rows[0], 0).wait_recv()
        near_w(q, z, outer_rows, 0).start()

        @pl.when(inner)
        def _():
            mid_w(q, z, inner_rows, 0).start()

    def w_own_outer(q):
        fetch_w(q, z, outer_rows[1], 1).wait_recv()
        near_w(q, z, outer_rows, 1).start()

    def w_own_inner(q):
        fetch_w(q, z, inner_rows[1], 1).wait_recv()
        near_w(q, z, inner_rows, 1).start()
        mid_w(q, z, inner_rows, 1).start()

    def w_lent(q):
        fetch_w(q, znear, inner_rows[2], 2).wait_recv()
        near_w(q, znear, inner_rows, 2).start()

    def w_borrowed(q):
        near_w(q, z, inner_rows, 2).wait_recv()
        mid_w(q, z, inner_rows, 2).start()

    def w_down(q, h):
        mid_w(q, last - z, inner_rows, h).wait_recv()
        near_w(q, last - z, inner_rows, h).start()

    def w_across(q, h):
        near_w(q, znear, outer_rows, h).wait_recv()
        mid_w(q, znear, outer_rows, h).start()

    def w_far(q, h):
        mid_w(q, last - znear, outer_rows, h).wait_recv()
        near_w(q, last - znear, outer_rows, h).start()

    def back_send(q, i):
        once("w", lambda: [load_w(c) for c in range(2 * STEPS)])
        c = chunk(q, order[i])
        if i > 0:
            @pl.when(outer)
            def _():
                parts = (None, inner_rows[:2], inner_rows, outer_rows)[i]
                for h in range(len(parts)):
                    near_w(q, order[i], parts, h).wait_recv()
        pbs[c] = jnp.dot(ogcat[q, rows:2 * rows, :], whalf[c], preferred_element_type=F32).astype(BF)
        send_pb(q, order[i]).start()

    def back_keep(q, i):
        c = chunk(q, order[i])
        pbo[c] = jnp.dot(ogcat[q, 0:rows, :], whalf[c], preferred_element_type=F32)

    def finish(q, i):
        c = chunk(q, order[i])
        send_pb(q, order[i]).wait_recv()
        positive = jnp.maximum(hpc[0, c].astype(F32), 0.0)
        hg_out[:, cut(c, fc)] = (2.0 * positive * (pbo[c] + pbr[c].astype(F32))).astype(BF)

    shared = {
        "sw": lambda q: fetch_w(q, z, outer_rows[0], 0).start(),
        "sog": lambda q, far: on_core(lambda v: send_og(q, og_part(q, far), v).start()),
        "shp": lambda q, k: send_hp(q, k).start(),
        "tr0": transpose_own, "ogr": og_relay, "ogt": og_whole,
        "gout": grad_send, "gown": grad_keep, "w1": w_own,
        "bk": back_send, "bko": back_keep, "fin": finish,
    }
    at_outer = {
        "za": z_outer_send, "zd": z_outer_last, "w1b": w_own_outer, "w1c": w_lent,
        "sw1": lambda q: fetch_w(q, z, outer_rows[1], 1).start(),
        "sw2": lambda q: fetch_w(q, znear, inner_rows[2], 2).start(),
    }
    at_inner = {
        "zb": z_inner_send, "zc": z_inner_last, "zg": grad_merge, "w1b": w_own_inner,
        "w4": w_borrowed, "w2a": w_down, "w2b": w_across, "w3": w_far,
        "sw1": lambda q: fetch_w(q, z, inner_rows[1], 1).start(),
    }

    def run_group(table, role, group):
        steps = [(table[name], args) for name, *args in group if name in table]
        if steps:
            @pl.when(role)
            def _():
                for act, args in steps:
                    act(*args)

    barrier = pltpu.get_barrier_semaphore()
    for peer in (apeer, bpeer, cpeer, znext):
        pl.semaphore_signal(barrier, inc=1, device_id=peer, device_id_type=MESH)

    @pl.when(inner)
    def _():
        pl.semaphore_signal(barrier, inc=1, device_id=zmid, device_id_type=MESH)

    for q, p in both:
        load_og(q, p).start()
    pl.semaphore_wait(barrier, jnp.where(outer, 4, 5))
    group = []
    started = False
    for step in PLAN:
        if step[0] in shared:
            run_group(at_outer, outer, group)
            run_group(at_inner, inner, group)
            group = []
            if not started and step[0] == "tr0":
                started = True
                for c in range(2 * STEPS):
                    load_hp(c).start()
                for c in range(2 * STEPS):
                    load_w(c).start()
            shared[step[0]](*step[1:])
        else:
            group.append(step)
    run_group(at_outer, outer, group)
    run_group(at_inner, inner, group)

    def og_sent(v):
        for q, p in both:
            send_og(q, p, v).wait_send()
            pass_og(q, p, v).wait_send()

    on_core(og_sent)
    for q in range(2):
        fetch_w(q, z, outer_rows[0], 0).wait_send()
        near_w(q, z, outer_rows, 0).wait_send()
        for k in range(count):
            send_hp(q, k).wait_send()
        for j in range(STEPS):
            send_pb(q, j).wait_send()
    pieces = [(q, k, h) for k in range(count) for q in range(2) for h in halves]
    for q, k, h in pieces:
        if k != VIA_Z:
            send_g(q, k, h).wait_send()

    @pl.when(outer)
    def _():
        for q in range(2):
            fetch_w(q, z, outer_rows[1], 1).wait_send()
            fetch_w(q, znear, inner_rows[2], 2).wait_send()
            near_w(q, z, outer_rows, 1).wait_send()
            near_w(q, znear, inner_rows, 2).wait_send()
            for h in halves:
                send_zg(q, h).wait_send()
        for q, k, h in pieces:
            send_z1(q, k, h).wait_send()

    @pl.when(inner)
    def _():
        for q in range(2):
            fetch_w(q, z, inner_rows[1], 1).wait_send()
            near_w(q, z, inner_rows, 1).wait_send()
            for h in range(3):
                mid_w(q, z, inner_rows, h).wait_send()
                near_w(q, last - z, inner_rows, h).wait_send()
            for h in range(2):
                mid_w(q, znear, outer_rows, h).wait_send()
                near_w(q, last - znear, outer_rows, h).wait_send()
            for h in halves:
                send_g(q, VIA_Z, h).wait_send()
        for q, k, h in pieces:
            send_z2(q, k, h).wait_send()
            send_z3(q, k, h).wait_send()


def put_kernel(hg, total, hg_out, tot_out, wide, sems):
    size = hg.shape[0] // PUTS
    tokens_all = size * PUTS * lax.axis_size("rep") * lax.axis_size("fs")
    copies = []
    for i in range(PUTS):
        span = pl.ds(i * size, size)
        copies.append(pltpu.make_async_copy(hg.at[span], hg_out.at[span], sems.at[1, i]))
        copies[-1].start()
        wide[span] = total[span].astype(F32) * (1.0 / math.sqrt(tokens_all))
        copies.append(pltpu.make_async_copy(wide.at[span], tot_out.at[span], sems.at[0, i]))
        copies[-1].start()
    for copy in copies:
        copy.wait()


def paired_body(hidden_pre, out_grad, down_weight):
    rows, ff = hidden_pre.shape
    depth = down_weight.shape[0]
    chunks = 2 * STEPS
    fc = ff // chunks
    count = len(PIECES)
    via = PIECES[VIA_Z][2] * fc // 2
    any_spec = pl.BlockSpec(memory_space=pl.ANY)
    vmem_spec = pl.BlockSpec(memory_space=pltpu.VMEM)

    def block(r, dtype):
        return pltpu.VMEM((chunks, r, fc), dtype)

    sem = pltpu.SemaphoreType.DMA
    hidden_grad, total = pl.pallas_call(
        kernel,
        out_shape=(jax.ShapeDtypeStruct((rows, ff), BF), jax.ShapeDtypeStruct((depth, ff), BF)),
        in_specs=[any_spec] * 3,
        out_specs=(vmem_spec, vmem_spec),
        scratch_shapes=[
            pltpu.VMEM((2, 2 * rows, 2 * depth), BF),
            pltpu.VMEM((2, 2 * depth, 2 * rows), BF),
            block(2 * depth, BF),
            pltpu.VMEM((2, chunks, rows, fc), BF),
            block(rows, BF), block(rows, BF), block(rows, F32),
            block(depth, BF), block(depth, BF), block(depth, F32),
            block(depth, BF), block(depth, BF), block(depth, BF), block(depth, BF),
            pltpu.VMEM((2, depth, via), F32), pltpu.VMEM((2, depth, via), BF),
            sem((2, 2)), sem((chunks,)), sem((chunks,)),
        ] + [sem((2, 2))] * 4 + [sem((2, 3))] * 2 + [sem((chunks, 3))] * 3 + [sem((chunks,))] * 2
        + [sem((2, count))] * 2 + [sem((2, count, PARTS))] * 8 + [sem((2, PARTS))] * 2,
        compiler_params=pltpu.CompilerParams(
            collective_id=0, has_side_effects=True, vmem_limit_bytes=48 * 1024 * 1024
        ),
    )(hidden_pre, out_grad, down_weight)
    return pl.pallas_call(
        put_kernel,
        out_shape=(jax.ShapeDtypeStruct((rows, ff), BF), jax.ShapeDtypeStruct((depth, ff), F32)),
        in_specs=[any_spec, vmem_spec],
        out_specs=(any_spec, any_spec),
        scratch_shapes=[pltpu.VMEM((depth, ff), F32), pltpu.SemaphoreType.DMA((2, PUTS))],
        compiler_params=pltpu.CompilerParams(vmem_limit_bytes=8 * 1024 * 1024),
    )(hidden_grad, total)


def solution(mesh):
    placed = (P(("rep", "fs"), "tp"), P(("rep", "fs"), None), P("fs", "tp"))
    two_by_two = mesh.shape["fs"] == 4 and mesh.shape["tp"] == 2 and mesh.shape["rep"] == 4
    return jax.shard_map(
        paired_body if two_by_two else plain_body,
        mesh=mesh,
        in_specs=placed,
        out_specs=(P(("rep", "fs"), "tp"), P("fs", "tp")),
        check_vma=False,
    )
```
